1024 devices in a mesh: sp: 16 (over x, core), dp: 64 (over z, y).
Axes of the slice: x: 8, y: 8, z: 8, core: 2. Of those that a mesh axis runs over, the one named last changes fastest.
Arguments:
- queries: bfloat16 [4096, 64, 512], P('sp', 'dp'), may hold values from -6 to 6
- head_keys: bfloat16 [4096, 64, 512], P('sp', 'dp'), may hold values from -6 to 6
- decay_preact: bfloat16 [4096, 64, 512], P('sp', 'dp'), may hold values from -3.2 to 3.2
- values: bfloat16 [4096, 64, 1024], P('sp', 'dp'), may hold values from -18 to 18
- extra_log_decay: float32 [256, 4096], P('dp', 'sp'), may hold values from -0.7 to 0
- decay_offset_bias: float32 [4, 128], replicated, may hold values from 0.3 to 8
- opening_state: float32 [64, 4, 128, 256], P('dp'), may hold values from -192 to 192
- output_norm_gain: float32 [256], replicated, may hold values from 0.1 to 1.9
- output_weight: bfloat16 [1024, 2048], P(None, 'dp'), may hold values from -0.1875 to 0.1875
Outputs:
- layer_out: bfloat16 [4096, 64, 2048], P('sp', 'dp')
The draws below stay inside these ranges and needn't reach their ends.
All inputs are finite; a program needn't handle non-finite values.
Results may differ from the reference program's by a relative error of at most 0.015.
Values may be sent and summed in bfloat16 or wider, within the bound.
No kernel may reach another device: no remote copies, remote signals or barrier semaphores. Data moves between devices by JAX's collectives and lax.ppermute only.
A program may use at most 64 MiB of HBM per device.

```python
import jax
import jax.numpy as jnp
from jax import lax

D = 2048
HEAD_COUNT = 4
KEY_CHANNELS = 128
DV = 256
BLOCK = 64
SEQ_TOK = 256
SEQUENCE_LENGTH = 4096
SEQUENCE_COUNT = 64
ITEMS = 256


def draw_decay_preact(key, part):
    folded = jax.random.fold_in(key, 11)
    first, second = jax.random.split(folded)
    data = 0.8 * jnp.clip(jax.random.normal(first, (SEQUENCE_LENGTH, SEQUENCE_COUNT, HEAD_COUNT, KEY_CHANNELS), jnp.float32), -3.0, 3.0)
    offsets = jax.random.uniform(second, (SEQUENCE_LENGTH // SEQ_TOK, SEQUENCE_COUNT, HEAD_COUNT), jnp.float32, -0.7, 0.7)
    offsets = jnp.repeat(offsets, SEQ_TOK, axis=0)[:, :, :, None]
    return (data + offsets).reshape(SEQUENCE_LENGTH, SEQUENCE_COUNT, HEAD_COUNT * KEY_CHANNELS).astype(jnp.bfloat16)


def draw_values(key, part):
    folded = jax.random.fold_in(key, 21)
    first = jax.random.fold_in(folded, 0)
    base = jnp.clip(jax.random.normal(first, (SEQUENCE_LENGTH, SEQUENCE_COUNT, HEAD_COUNT * DV), jnp.float32), -6.0, 6.0)
    return base.astype(jnp.bfloat16)


def draw_extra_log_decay(key, part):
    folded = jax.random.fold_in(key, 31)
    first, second = jax.random.split(folded)
    hits = jax.random.randint(first, (ITEMS, SEQUENCE_LENGTH), 0, max(SEQUENCE_LENGTH // 3, 1)) == 0
    depth = jax.random.uniform(second, (ITEMS, SEQUENCE_LENGTH), jnp.float32, jnp.log(0.5), jnp.log(0.8))
    return jnp.where(hits, depth, jnp.float32(0.0)).astype(jnp.float32)


def draw_decay_offset_bias(key, part):
    folded = jax.random.fold_in(key, 41)
    first, second, third = jax.random.split(folded, 3)
    quick = jax.random.randint(first, (HEAD_COUNT, KEY_CHANNELS), 0, 2) == 0
    slow_rate = jnp.exp(jax.random.uniform(second, (HEAD_COUNT, KEY_CHANNELS), jnp.float32, jnp.log(0.15), jnp.log(0.6))) / SEQUENCE_LENGTH
    slow_level = -jnp.log(16.0 * slow_rate)
    quick_level = jax.random.uniform(third, (HEAD_COUNT, KEY_CHANNELS), jnp.float32, 0.35, 1.75)
    return jnp.where(quick, quick_level, slow_level).astype(jnp.float32)


def levels(stream_key, dims, cuts, smallest, largest):
    loudness, own = 1.0, jax.random.fold_in(stream_key, 6)
    for axis_at, shards_of in cuts:
        draws = jnp.exp(jax.random.uniform(jax.random.fold_in(own, axis_at), (shards_of,), jnp.float32, smallest / len(cuts), largest / len(cuts)))
        loudness = loudness * jnp.repeat(draws, dims[axis_at] // shards_of).reshape([-1 if axis == axis_at else 1 for axis in range(len(dims))])
    return loudness


def scatter_about(rng, shape, spread, bound, cuts=(), held_as=jnp.bfloat16):
    result = jax.random.normal(rng, shape, jnp.float32) * spread
    if len(cuts) > 0:
        result = levels(rng, shape, cuts, -0.22, 0.18) * result
    return jnp.clip(result, min=-bound, max=bound).astype(held_as)


def setup_inputs(seed: int = 0) -> dict:
    keys = jax.random.split(jax.random.key(seed), 10)
    queries = scatter_about(keys[0], (SEQUENCE_LENGTH, SEQUENCE_COUNT, HEAD_COUNT * KEY_CHANNELS), 1.0, 6.0, ((0, 16), (1, 64)))
    head_keys = scatter_about(keys[1], (SEQUENCE_LENGTH, SEQUENCE_COUNT, HEAD_COUNT * KEY_CHANNELS), 1.0, 6.0, ((0, 16), (1, 64)))
    decay_preact = draw_decay_preact(jax.random.fold_in(keys[9], 71), 0)
    values = draw_values(jax.random.fold_in(keys[9], 71), 0)
    extra_log_decay = draw_extra_log_decay(jax.random.fold_in(keys[9], 71), 0)
    decay_offset_bias = draw_decay_offset_bias(jax.random.fold_in(keys[9], 71), 0)
    opening_state = scatter_about(keys[6], (SEQUENCE_COUNT, HEAD_COUNT, KEY_CHANNELS, DV), ((SEQUENCE_LENGTH // 4) ** 0.5), 192.0, ((0, 64),), jnp.float32)
    output_norm_gain = jnp.clip(1.0 + 0.18 * jax.random.normal(keys[7], (DV,), jnp.float32), 0.1, 1.9)
    output_weight = scatter_about(keys[8], (HEAD_COUNT * DV, D), (HEAD_COUNT * DV) ** -0.5, 0.1875, ((1, 64),))
    return {"queries": queries, "head_keys": head_keys, "decay_preact": decay_preact, "values": values, "extra_log_decay": extra_log_decay, "decay_offset_bias": decay_offset_bias, "opening_state": opening_state, "output_norm_gain": output_norm_gain, "output_weight": output_weight}


gate_norm_term = 16.0
norm_eps = 1e-05

def blockwise(query_matrix, key_matrix, value_matrix, decay_logarithm, entry_state):
    length, group_count, key_dim = query_matrix.shape
    value_dim = value_matrix.shape[-1]
    blocks = length // BLOCK

    def by_block(tensor):
        return tensor.reshape(blocks, BLOCK, group_count, tensor.shape[-1])
    cumulative = jnp.cumsum(by_block(decay_logarithm), axis=1)
    block_end = cumulative[:, -1]
    q_in = by_block(query_matrix) * jnp.exp(cumulative)
    k_in = by_block(key_matrix) * jnp.exp(-cumulative)
    k_out = by_block(key_matrix) * jnp.exp(block_end[:, None] - cumulative)
    block_values = by_block(value_matrix)
    causal = jnp.tril(jnp.ones((BLOCK, BLOCK), dtype=bool))
    scores = jnp.einsum('ntid,nsid->nits', q_in, k_in, precision=lax.Precision.HIGHEST)
    scores = jnp.where(causal, scores, jnp.float32(0.0))
    within = jnp.einsum('nits,nsie->ntie', scores, block_values, precision=lax.Precision.HIGHEST)
    summary = jnp.einsum('nsid,nsie->nide', k_out, block_values, precision=lax.Precision.HIGHEST)

    def advance(carried, input_arrays):
        summand, decay_end = input_arrays
        return (carried * jnp.exp(decay_end)[..., None] + summand, carried)
    _, starts = lax.scan(advance, entry_state, (summary, block_end))
    carried_out = jnp.einsum('ntid,nide->ntie', q_in, starts, precision=lax.Precision.HIGHEST)
    return (within + carried_out).reshape(length, group_count, value_dim)

def reference(queries, head_keys, decay_preact, values, extra_log_decay, decay_offset_bias, opening_state, output_norm_gain, output_weight):

    def sequence_wise(input_arrays):
        query_matrix, key_matrix, logit_matrix, value_matrix, decay_spikes, entry_state = input_arrays
        decay_logarithm = jax.nn.log_sigmoid(logit_matrix.astype(jnp.float32).reshape(SEQUENCE_LENGTH, HEAD_COUNT, KEY_CHANNELS) + decay_offset_bias[None]) / gate_norm_term + decay_spikes.T[:, :, None]
        scaled = query_matrix.astype(jnp.float32).reshape(SEQUENCE_LENGTH, HEAD_COUNT, KEY_CHANNELS) * KEY_CHANNELS ** (-0.5)
        output = blockwise(scaled, key_matrix.astype(jnp.float32).reshape(SEQUENCE_LENGTH, HEAD_COUNT, KEY_CHANNELS), value_matrix.astype(jnp.float32).reshape(SEQUENCE_LENGTH, HEAD_COUNT, DV), decay_logarithm, entry_state)
        normed = (output * lax.rsqrt(lax.optimization_barrier(jnp.mean(output * output, axis=-1, keepdims=True)) + norm_eps) * output_norm_gain).astype(jnp.bfloat16)
        return jnp.dot(normed.reshape(SEQUENCE_LENGTH, HEAD_COUNT * DV), output_weight, preferred_element_type=jnp.float32).astype(jnp.bfloat16)
    mapped_result = lax.map(sequence_wise, (jnp.moveaxis(queries, 1, 0), jnp.moveaxis(head_keys, 1, 0), jnp.moveaxis(decay_preact, 1, 0), jnp.moveaxis(values, 1, 0), extra_log_decay.reshape(SEQUENCE_COUNT, HEAD_COUNT, SEQUENCE_LENGTH), opening_state))
    return jnp.moveaxis(mapped_result, 0, 1)
```

```python
import jax
import jax.numpy as jnp
from jax import lax
from jax.experimental import pallas as pl
from jax.experimental.pallas import tpu as pltpu
from jax.sharding import PartitionSpec as P

BLOCK = 64
gate_norm_term = 16.0
norm_eps = 1e-05
F32 = jnp.float32
BF16 = jnp.bfloat16
VMEM = pl.BlockSpec(memory_space=pltpu.VMEM)


def dot(a, b, dims=(((1,), (0,)), ((), ()))):
    return lax.dot_general(a, b, dims, preferred_element_type=F32)


NT = (((1,), (1,)), ((), ()))
TN = (((0,), (0,)), ((), ()))


def summary_kernel(k_ref, x_ref, v_ref, extra_ref, bias_ref, send_ref, cum_ref):
    tok = k_ref.shape[0]
    heads, kd = bias_ref.shape
    vd = v_ref.shape[1] // heads
    per, rows = send_ref.shape[0] // heads, kd * heads // send_ref.shape[0]
    spikes = jnp.transpose(extra_ref[...])
    tri = (
        lax.broadcasted_iota(jnp.int32, (tok, tok), 0)
        >= lax.broadcasted_iota(jnp.int32, (tok, tok), 1)
    ).astype(BF16)
    for h in range(heads):
        cols = slice(h * kd, (h + 1) * kd)
        x = x_ref[:, cols].astype(F32) + bias_ref[h : h + 1, :]
        log_sig = jnp.minimum(x, 0.0) - jnp.log(1.0 + jnp.exp(-jnp.abs(x)))
        decay = log_sig * (1.0 / gate_norm_term) + spikes[:, h : h + 1]
        high = decay.astype(BF16)
        rest = decay - high.astype(F32)
        mid = rest.astype(BF16)
        low = (rest - mid.astype(F32)).astype(BF16)
        cum = dot(tri, high) + dot(tri, mid) + dot(tri, low)
        cum_ref[:, cols] = cum
        total = cum[tok - 1 : tok, :]
        k_out = (k_ref[:, cols].astype(F32) * jnp.exp(total - cum)).astype(BF16)
        final = dot(k_out, v_ref[:, h * vd : (h + 1) * vd], TN).astype(BF16)
        rate = jnp.broadcast_to(jnp.exp(total), (8, kd))
        for r in range(per):
            send_ref[h * per + r, 0:rows, :] = final[r * rows : (r + 1) * rows, :]
            turned = pltpu.roll(rate, (kd - r * rows) % kd, 1) if r else rate
            coarse = turned.astype(BF16)
            fine = (turned - coarse.astype(F32)).astype(BF16)
            send_ref[h * per + r, rows : rows + 8, :] = jnp.concatenate([coarse, fine], axis=1)


def inside_kernel(q_ref, k_ref, v_ref, cum_ref, inside_ref, far_ref):
    tok, width = q_ref.shape
    kd = 128
    heads = width // kd
    vd = v_ref.shape[1] // heads
    scale = kd ** (-0.5)
    for h in range(heads):
        cols = slice(h * kd, (h + 1) * kd)
        vcols = slice(h * vd, (h + 1) * vd)
        for i in range(tok // BLOCK):
            lo, hi = i * BLOCK, (i + 1) * BLOCK
            q = q_ref[lo:hi, cols].astype(F32) * scale
            cum = cum_ref[lo:hi, cols]
            far_ref[lo:hi, cols] = (q * jnp.exp(cum)).astype(BF16)
            if i:
                base = cum_ref[lo - 1 : lo, cols]
                q_in = (q * jnp.exp(cum - base)).astype(BF16)
                k_in = (k_ref[0:hi, cols].astype(F32) * jnp.exp(base - cum_ref[0:hi, cols])).astype(BF16)
            else:
                q_in = (q * jnp.exp(cum)).astype(BF16)
                k_in = (k_ref[0:hi, cols].astype(F32) * jnp.exp(-cum)).astype(BF16)
            scores = dot(q_in, k_in, NT)
            seen = (
                lax.broadcasted_iota(jnp.int32, (BLOCK, hi), 0) + lo
                >= lax.broadcasted_iota(jnp.int32, (BLOCK, hi), 1)
            )
            scores = jnp.where(seen, scores, 0.0).astype(BF16)
            inside_ref[lo:hi, vcols] = dot(scores, v_ref[0:hi, vcols])


def chain_kernel(who_ref, got_ref, open_ref, out_ref):
    group = got_ref.shape[0]
    rows = out_ref.shape[1]
    state = open_ref[...]
    where = lax.broadcasted_iota(jnp.int32, (8, 128), 0)
    parts = []
    for g in range(group // 8):
        table = jnp.zeros((8, 128), F32)
        for d in range(8):
            pair = got_ref[g * 8 + d, rows : rows + 8, :].astype(F32)
            table = jnp.where(where == d, pair[:, 0:128] + pair[:, 128:256], table)
        parts.append(table)
    rates = jnp.transpose(jnp.concatenate(parts, axis=0))
    for d in range(group):
        out_ref[d] = state.astype(BF16)
        if d < group - 1:
            state = rates[0:rows, d : d + 1] * state + got_ref[d, 0:rows, :].astype(F32)


def project_kernel(who_ref, inside_ref, far_ref, start_ref, gain_ref, mine_ref, other_ref, out_ref, normed):
    heads = 4
    kd, vd = far_ref.shape[1] // heads, start_ref.shape[1]
    half = mine_ref.shape[1]

    @pl.when(pl.program_id(0) == 0)
    def _():
        for h in range(heads):
            o = inside_ref[:, h * vd : (h + 1) * vd] + dot(
                far_ref[:, h * kd : (h + 1) * kd], start_ref[h * kd : (h + 1) * kd, :]
            )
            spread = lax.rsqrt(jnp.mean(o * o, axis=-1, keepdims=True) + norm_eps)
            normed[:, h * vd : (h + 1) * vd] = (o * spread * gain_ref[...]).astype(BF16)

    core = who_ref[1]
    first = normed[:, pl.ds(pl.multiple_of(core * half, half), half)]
    second = normed[:, pl.ds(pl.multiple_of((1 - core) * half, half), half)]
    out_ref[...] = (dot(first, mine_ref[...], NT) + dot(second, other_ref[...], NT)).astype(BF16)


def on_device(
    queries,
    head_keys,
    decay_preact,
    values,
    extra_log_decay,
    decay_offset_bias,
    opening_state,
    output_norm_gain,
    output_weight,
):
    tok, seqs, width = queries.shape
    heads, kd = decay_offset_bias.shape
    vd = output_norm_gain.shape[0]
    group = lax.axis_size("sp")
    columns_group = lax.axis_size("dp")
    share = output_weight.shape[1]
    model = share * columns_group
    rows = heads * kd // group
    sp = lax.axis_index("sp")
    core = lax.rem(sp, 2)
    who = jnp.stack([sp, core]).astype(jnp.int32)
    half = heads * vd // 2

    q = queries.reshape(tok, width)
    k = head_keys.reshape(tok, width)
    x = decay_preact.reshape(tok, width)
    v = values.reshape(tok, heads * vd)
    opening = opening_state.reshape(heads * kd, vd)

    part = lax.dynamic_slice_in_dim(output_weight.T, core * half, half, 1)
    spread_part = jnp.broadcast_to(part[None], (columns_group, share, half))
    mine = lax.all_to_all(spread_part, "dp", 0, 0, tiled=True).reshape(model, half)
    other = lax.ppermute(mine, "sp", [(i, i ^ 1) for i in range(group)])

    send, cum = pl.pallas_call(
        summary_kernel,
        out_shape=(
            jax.ShapeDtypeStruct((group, rows + 8, vd), BF16),
            jax.ShapeDtypeStruct((tok, width), F32),
        ),
        in_specs=[VMEM] * 5,
        out_specs=(VMEM, VMEM),
        cost_estimate=pl.CostEstimate(flops=10**9, bytes_accessed=2 * 10**6, transcendentals=10**6),
        name="summary",
    )(k, x, v, extra_log_decay, decay_offset_bias)

    got = lax.all_to_all(send, "sp", 0, 0, tiled=True)

    inside, far = pl.pallas_call(
        inside_kernel,
        out_shape=(
            jax.ShapeDtypeStruct((tok, heads * vd), F32),
            jax.ShapeDtypeStruct((tok, width), BF16),
        ),
        in_specs=[VMEM] * 4,
        out_specs=(VMEM, VMEM),
        cost_estimate=pl.CostEstimate(flops=3 * 10**9, bytes_accessed=3 * 10**6, transcendentals=10**6),
        name="inside",
    )(q, k, v, cum)

    starts = pl.pallas_call(
        chain_kernel,
        out_shape=jax.ShapeDtypeStruct((group, rows, vd), BF16),
        grid_spec=pltpu.PrefetchScalarGridSpec(
            num_scalar_prefetch=1,
            grid=(1,),
            in_specs=[
                pl.BlockSpec((group, rows + 8, vd), lambda i, who: (0, 0, 0)),
                pl.BlockSpec((rows, vd), lambda i, who: (who[0], 0)),
            ],
            out_specs=pl.BlockSpec((group, rows, vd), lambda i, who: (0, 0, 0)),
        ),
        name="chain",
    )(who, got, opening)

    start = lax.all_to_all(starts, "sp", 0, 0, tiled=True).reshape(heads * kd, vd)

    tile = 512
    out = pl.pallas_call(
        project_kernel,
        out_shape=jax.ShapeDtypeStruct((tok, model), BF16),
        grid_spec=pltpu.PrefetchScalarGridSpec(
            num_scalar_prefetch=1,
            grid=(model // tile,),
            in_specs=[
                pl.BlockSpec((tok, heads * vd), lambda i, who: (0, 0)),
                pl.BlockSpec((tok, width), lambda i, who: (0, 0)),
                pl.BlockSpec((heads * kd, vd), lambda i, who: (0, 0)),
                pl.BlockSpec((1, vd), lambda i, who: (0, 0)),
                pl.BlockSpec((tile, half), lambda i, who: (i, 0)),
                pl.BlockSpec((tile, half), lambda i, who: (i, 0)),
            ],
            out_specs=pl.BlockSpec((tok, tile), lambda i, who: (0, i)),
            scratch_shapes=[pltpu.VMEM((tok, heads * vd), BF16)],
        ),
        name="project",
    )(who, inside, far, start, output_norm_gain.reshape(1, vd), mine, other)
    return out.reshape(tok, seqs, model)


def solution(mesh):
    return jax.shard_map(
        on_device,
        mesh=mesh,
        in_specs=(
            P("sp", "dp", None),
            P("sp", "dp", None),
            P("sp", "dp", None),
            P("sp", "dp", None),
            P("dp", "sp"),
            P(),
            P("dp", None, None, None),
            P(),
            P(None, "dp"),
        ),
        out_specs=P("sp", "dp", None),
        check_vma=False,
    )
```

```python
import jax
import jax.numpy as jnp
from jax import lax
from jax.experimental import pallas as pl
from jax.experimental.pallas import tpu as pltpu
from jax.sharding import PartitionSpec as P


BLOCK = 64
gate_norm_term = 16.0
norm_eps = 1e-05
F32 = jnp.float32
BF16 = jnp.bfloat16
VMEM = pl.BlockSpec(memory_space=pltpu.VMEM)
HBM = pl.BlockSpec(memory_space=pltpu.HBM)
SMEM = pl.BlockSpec(memory_space=pltpu.SMEM)
SIDE = 8
TILES = 4


def dot(a, b, dims=(((1,), (0,)), ((), ()))):
    return lax.dot_general(a, b, dims, preferred_element_type=F32)


NT = (((1,), (1,)), ((), ()))
TN = (((0,), (0,)), ((), ()))


def fetch(sems, *pairs):
    copies = [pltpu.make_async_copy(a, b, sems.at[n]) for n, (a, b) in enumerate(pairs)]
    for c in copies:
        c.start()
    return copies


def spread_kernel(who_ref, weight_hbm, out_ref, quarters, sems):
    core = who_ref[1]
    width = out_ref.shape[2]
    pairs = []
    for c in range(4):
        first = pl.multiple_of((core * 4 + c) * width, width)
        pairs.append((weight_hbm.at[:, pl.ds(first, width)], quarters.at[c]))
    for c in fetch(sems, *pairs):
        c.wait()
    for d in range(out_ref.shape[0]):
        out_ref[d] = quarters[(d % SIDE + 2 * (d // SIDE)) % 4]


def summary_kernel(k_hbm, x_hbm, v_hbm, extra_hbm, bias_hbm, send_ref, cum_ref, k_ref, x_ref, v_ref, extra_ref, bias_ref, sems):
    get_x, get_extra, get_bias, get_k, get_v = fetch(
        sems, (x_hbm, x_ref), (extra_hbm, extra_ref), (bias_hbm, bias_ref), (k_hbm, k_ref), (v_hbm, v_ref)
    )
    tok = k_ref.shape[0]
    heads, kd = bias_ref.shape
    vd = v_ref.shape[1] // heads
    per, rows = send_ref.shape[0] // heads, kd * heads // send_ref.shape[0]
    wide = vd // kd
    tri = (
        lax.broadcasted_iota(jnp.int32, (tok, tok), 0)
        >= lax.broadcasted_iota(jnp.int32, (tok, tok), 1)
    ).astype(BF16)
    odd = lax.broadcasted_iota(jnp.int32, (8, kd), 0) % 2 == 1
    get_extra.wait()
    spikes = jnp.transpose(extra_ref[...])
    get_bias.wait()
    get_x.wait()
    for h in range(heads):
        cols = slice(h * kd, (h + 1) * kd)
        x = x_ref[:, cols].astype(F32) + bias_ref[h : h + 1, :]
        log_sig = jnp.minimum(x, 0.0) - jnp.log(1.0 + jnp.exp(-jnp.abs(x)))
        decay = log_sig * (1.0 / gate_norm_term) + spikes[:, h : h + 1]
        high = decay.astype(BF16)
        rest = decay - high.astype(F32)
        mid = rest.astype(BF16)
        low = (rest - mid.astype(F32)).astype(BF16)
        cum = dot(tri, high) + dot(tri, mid) + dot(tri, low)
        cum_ref[:, cols] = cum
        total = cum[tok - 1 : tok, :]
        if h == 0:
            get_k.wait()
            get_v.wait()
        k_out = (k_ref[:, cols].astype(F32) * jnp.exp(total - cum)).astype(BF16)
        final = dot(k_out, v_ref[:, h * vd : (h + 1) * vd], TN).astype(BF16)
        rate = jnp.broadcast_to(jnp.exp(total), (8, kd))
        for r in range(per):
            for w in range(wide):
                send_ref[h * per + r, w * rows : (w + 1) * rows, :] = final[
                    r * rows : (r + 1) * rows, w * kd : (w + 1) * kd
                ]
            turned = pltpu.roll(rate, (kd - r * rows) % kd, 1) if r else rate
            coarse = turned.astype(BF16).astype(F32)
            send_ref[h * per + r, wide * rows : wide * rows + 8, :] = jnp.where(
                odd, turned - coarse, coarse
            ).astype(BF16)


def inside_kernel(
    who_ref, cum_ref, q_hbm, k_hbm, v_hbm, open_hbm, inside_ref, far_ref, open_ref, q_ref, k_ref, v_ref, sems
):
    mine = open_ref.shape[0]
    first = pl.multiple_of(who_ref[0] * mine, mine)
    for c in fetch(
        sems, (q_hbm, q_ref), (k_hbm, k_ref), (v_hbm, v_ref), (open_hbm.at[pl.ds(first, mine), :], open_ref)
    ):
        c.wait()
    tok, width = q_ref.shape
    kd = 128
    heads = width // kd
    vd = v_ref.shape[1] // heads
    scale = kd ** (-0.5)
    for h in range(heads):
        cols = slice(h * kd, (h + 1) * kd)
        vcols = slice(h * vd, (h + 1) * vd)
        for i in range(tok // BLOCK):
            lo, hi = i * BLOCK, (i + 1) * BLOCK
            q = q_ref[lo:hi, cols].astype(F32) * scale
            cum = cum_ref[lo:hi, cols]
            far_ref[lo:hi, cols] = (q * jnp.exp(cum)).astype(BF16)
            if i:
                base = cum_ref[lo - 1 : lo, cols]
                q_in = (q * jnp.exp(cum - base)).astype(BF16)
                k_in = (k_ref[0:hi, cols].astype(F32) * jnp.exp(base - cum_ref[0:hi, cols])).astype(BF16)
            else:
                q_in = (q * jnp.exp(cum)).astype(BF16)
                k_in = (k_ref[0:hi, cols].astype(F32) * jnp.exp(-cum)).astype(BF16)
            scores = dot(q_in, k_in, NT)
            seen = (
                lax.broadcasted_iota(jnp.int32, (BLOCK, hi), 0) + lo
                >= lax.broadcasted_iota(jnp.int32, (BLOCK, hi), 1)
            )
            scores = jnp.where(seen, scores, 0.0).astype(BF16)
            inside_ref[lo:hi, vcols] = dot(scores, v_ref[0:hi, vcols])


def chain_kernel(got_ref, open_ref, out_ref):
    group = got_ref.shape[0]
    rows, vd = open_ref.shape
    wide = vd // 128
    where = lax.broadcasted_iota(jnp.int32, (8, 128), 0)
    parts = []
    for g in range(group // 8):
        table = jnp.zeros((8, 128), F32)
        for d in range(8):
            pair = got_ref[g * 8 + d, wide * rows : wide * rows + 8, :].astype(F32)
            table = jnp.where(where == d, pair + pltpu.roll(pair, 1, 0), table)
        parts.append(table)
    rates = jnp.transpose(jnp.concatenate(parts, axis=0))
    states = [open_ref[:, w * 128 : (w + 1) * 128] for w in range(wide)]
    for d in range(group):
        rate = jnp.broadcast_to(rates[0:rows, d : d + 1], (rows, 128))
        for w in range(wide):
            out_ref[d, :, w * 128 : (w + 1) * 128] = states[w].astype(BF16)
            states[w] = rate * states[w] + got_ref[d, w * rows : (w + 1) * rows, :].astype(F32)


def project_kernel(who_ref, inside_ref, far_ref, start_ref, *refs):
    gain_hbm, mine, other, out_hbm = refs[0], refs[1:5], refs[5], refs[6]
    normed, weight, gain_ref, tiles, in_sems, out_sems = refs[7:]
    core, color = who_ref[1], who_ref[2]
    half = normed.shape[1] // 2
    piece = half // 4
    model = weight.shape[0]
    heads = 4
    kd, vd = far_ref.shape[1] // heads, start_ref.shape[1]
    halves = TILES
    rows = model // halves
    pairs = [(gain_hbm, gain_ref)]
    for part in range(halves):
        span = pl.ds(part * rows, rows)
        for n in range(4):
            at = lax.rem(color + n, 4) * piece
            for base, src in ((core * half, mine[n]), ((1 - core) * half, other.at[n])):
                to = pl.ds(pl.multiple_of(base + at, piece), piece)
                pairs.append((src.at[span, :], weight.at[span, to]))
    copies = fetch(in_sems, *pairs)
    copies[0].wait()
    for h in range(heads):
        o = inside_ref[:, h * vd : (h + 1) * vd] + dot(
            far_ref[:, h * kd : (h + 1) * kd], start_ref[h * kd : (h + 1) * kd, :]
        )
        spread = lax.rsqrt(jnp.mean(o * o, axis=-1, keepdims=True) + norm_eps)
        normed[:, h * vd : (h + 1) * vd] = (o * spread * gain_ref[...]).astype(BF16)
    tile = model // TILES
    outs = []
    for t in range(TILES):
        if t % (TILES // halves) == 0:
            part = t // (TILES // halves)
            for c in copies[1 + 8 * part : 9 + 8 * part]:
                c.wait()
        tiles[t] = dot(normed[...], weight[t * tile : (t + 1) * tile, :], NT).astype(BF16)
        c = pltpu.make_async_copy(tiles.at[t], out_hbm.at[:, pl.ds(t * tile, tile)], out_sems.at[t])
        c.start()
        outs.append(c)
    for c in outs:
        c.wait()


def hbm(*arrays):
    return [pltpu.with_memory_space_constraint(a, pltpu.HBM) for a in arrays]


def vmem(*arrays):
    return [pltpu.with_memory_space_constraint(a, pltpu.VMEM) for a in arrays]


def params(mib):
    return pltpu.CompilerParams(vmem_limit_bytes=mib * 2**20)


def cost(flops):
    return pl.CostEstimate(flops=flops, bytes_accessed=10**6, transcendentals=0)


def on_device(
    queries,
    head_keys,
    decay_preact,
    values,
    extra_log_decay,
    decay_offset_bias,
    opening_state,
    output_norm_gain,
    output_weight,
):
    tok, seqs, width = queries.shape
    heads, kd = decay_offset_bias.shape
    vd = output_norm_gain.shape[0]
    group = lax.axis_size("sp")
    plane = lax.axis_size("dp")
    share = output_weight.shape[1]
    model = share * plane
    piece = heads * vd // 8
    rows = heads * kd // group
    packed = rows * vd // 128 + 8
    sp, dp = lax.axis_index("sp"), lax.axis_index("dp")
    z, y = lax.div(dp, SIDE), lax.rem(dp, SIDE)
    who = jnp.stack([sp, lax.rem(sp, 2), lax.rem(y + 2 * z, 4), z]).astype(jnp.int32)
    dma = pltpu.SemaphoreType.DMA

    q = queries.reshape(tok, width)
    k = head_keys.reshape(tok, width)
    x = decay_preact.reshape(tok, width)
    v = values.reshape(tok, heads * vd)
    opening = opening_state.reshape(heads * kd, vd)

    def from_offset(dz, dy):
        return [
            (((i + dz) % SIDE) * SIDE + (j + dy) % SIDE, i * SIDE + j)
            for i in range(plane // SIDE)
            for j in range(SIDE)
        ]

    spread = pl.pallas_call(
        spread_kernel,
        out_shape=pltpu.VMEM((plane, share, piece), BF16),
        in_specs=[SMEM, HBM],
        out_specs=VMEM,
        scratch_shapes=[pltpu.VMEM((4, share, piece), BF16), dma((4,))],
        compiler_params=params(4),
        cost_estimate=cost(10**6),
        name="spread",
    )(who, *hbm(output_weight.T))
    eighth = lax.all_to_all(spread, "dp", 0, 0, tiled=True).reshape(model, piece)
    mine = [eighth]
    for o in ((0, 1), (1, 0), (0, -1)):
        mine.append(lax.ppermute(eighth, "dp", from_offset(*o)))
    stacked = jnp.stack(mine)
    other = lax.ppermute(stacked, "sp", [(i, i ^ 1) for i in range(group)])

    send, cum = pl.pallas_call(
        summary_kernel,
        out_shape=(
            pltpu.VMEM((group, packed, 128), BF16),
            pltpu.VMEM((tok, width), F32),
        ),
        in_specs=[HBM] * 5,
        out_specs=(VMEM, VMEM),
        scratch_shapes=[
            pltpu.VMEM((tok, width), BF16),
            pltpu.VMEM((tok, width), BF16),
            pltpu.VMEM((tok, heads * vd), BF16),
            pltpu.VMEM(extra_log_decay.shape, F32),
            pltpu.VMEM((heads, kd), F32),
            dma((5,)),
        ],
        compiler_params=params(16),
        cost_estimate=cost(3 * 10**8),
        name="summary",
    )(*hbm(k, x, v, extra_log_decay, decay_offset_bias))

    got = lax.all_to_all(send, "sp", 0, 0, tiled=True)

    inside, far, own_opening = pl.pallas_call(
        inside_kernel,
        out_shape=(
            pltpu.VMEM((tok, heads * vd), F32),
            pltpu.VMEM((tok, width), BF16),
            pltpu.VMEM((rows, vd), F32),
        ),
        in_specs=[SMEM, VMEM] + [HBM] * 4,
        out_specs=(VMEM, VMEM, VMEM),
        scratch_shapes=[
            pltpu.VMEM((tok, width), BF16),
            pltpu.VMEM((tok, width), BF16),
            pltpu.VMEM((tok, heads * vd), BF16),
            dma((4,)),
        ],
        compiler_params=params(16),
        cost_estimate=cost(3 * 10**8),
        name="inside",
    )(who, *vmem(cum), *hbm(q, k, v, opening))

    starts = pl.pallas_call(
        chain_kernel,
        out_shape=pltpu.VMEM((group, rows, vd), BF16),
        in_specs=[VMEM, VMEM],
        out_specs=VMEM,
        compiler_params=params(8),
        cost_estimate=cost(10**7),
        name="chain",
    )(*vmem(got, own_opening))

    start = lax.all_to_all(starts, "sp", 0, 0, tiled=True).reshape(heads * kd, vd)

    out = pl.pallas_call(
        project_kernel,
        out_shape=jax.ShapeDtypeStruct((tok, model), BF16),
        in_specs=[SMEM] + [VMEM] * 3 + [HBM] * 6,
        out_specs=HBM,
        scratch_shapes=[
            pltpu.VMEM((tok, heads * vd), BF16),
            pltpu.VMEM((model, heads * vd), BF16),
            pltpu.VMEM((1, vd), F32),
            pltpu.VMEM((TILES, tok, model // TILES), BF16),
            dma((1 + 8 * TILES,)),
            dma((TILES,)),
        ],
        compiler_params=params(24),
        cost_estimate=cost(10**9),
        name="project",
    )(who, *vmem(inside, far, start), *hbm(output_norm_gain.reshape(1, vd), *mine, other))
    return out.reshape(tok, seqs, model)


def solution(mesh):
    return jax.shard_map(
        on_device,
        mesh=mesh,
        in_specs=(
            P("sp", "dp", None),
            P("sp", "dp", None),
            P("sp", "dp", None),
            P("sp", "dp", None),
            P("dp", "sp"),
            P(),
            P("dp", None, None, None),
            P(),
            P(None, "dp"),
        ),
        out_specs=P("sp", "dp", None),
        check_vma=False,
    )
```

```python
import jax
import jax.numpy as jnp
from jax import lax
from jax.experimental import pallas as pl
from jax.experimental.pallas import tpu as pltpu
from jax.sharding import PartitionSpec as P


BLOCK = 64
gate_norm_term = 16.0
norm_eps = 1e-05
F32 = jnp.float32
BF16 = jnp.bfloat16
VMEM = pl.BlockSpec(memory_space=pltpu.VMEM)
HBM = pl.BlockSpec(memory_space=pltpu.HBM)
SMEM = pl.BlockSpec(memory_space=pltpu.SMEM)
SIDE = 8
TILES = 4


def dot(a, b, dims=(((1,), (0,)), ((), ()))):
    return lax.dot_general(a, b, dims, preferred_element_type=F32)


NT = (((1,), (1,)), ((), ()))
TN = (((0,), (0,)), ((), ()))


def fetch(sems, *pairs):
    copies = [pltpu.make_async_copy(a, b, sems.at[n]) for n, (a, b) in enumerate(pairs)]
    for c in copies:
        c.start()
    return copies


def spread_kernel(who_ref, weight_hbm, out_ref, quarters, sems):
    core = who_ref[1]
    width = out_ref.shape[2]
    pairs = []
    for c in range(4):
        first = pl.multiple_of((core * 4 + c) * width, width)
        pairs.append((weight_hbm.at[:, pl.ds(first, width)], quarters.at[c]))
    for c in fetch(sems, *pairs):
        c.wait()
    for d in range(out_ref.shape[0]):
        out_ref[d] = quarters[(d % SIDE + 2 * (d // SIDE)) % 4]


def summary_kernel(k_hbm, x_hbm, v_hbm, extra_hbm, bias_hbm, send_ref, cum_ref, k_ref, x_ref, v_ref, extra_ref, bias_ref, sems):
    get_x, get_extra, get_bias, get_k, get_v = fetch(
        sems, (x_hbm, x_ref), (extra_hbm, extra_ref), (bias_hbm, bias_ref), (k_hbm, k_ref), (v_hbm, v_ref)
    )
    tok = k_ref.shape[0]
    heads, kd = bias_ref.shape
    vd = v_ref.shape[1] // heads
    per, rows = send_ref.shape[0] // heads, kd * heads // send_ref.shape[0]
    wide = vd // kd
    tri = (
        lax.broadcasted_iota(jnp.int32, (tok, tok), 0)
        >= lax.broadcasted_iota(jnp.int32, (tok, tok), 1)
    ).astype(BF16)
    odd = lax.broadcasted_iota(jnp.int32, (8, kd), 0) % 2 == 1
    get_extra.wait()
    spikes = jnp.transpose(extra_ref[...])
    get_bias.wait()
    get_x.wait()
    for h in range(heads):
        cols = slice(h * kd, (h + 1) * kd)
        x = x_ref[:, cols].astype(F32) + bias_ref[h : h + 1, :]
        log_sig = jnp.minimum(x, 0.0) - jnp.log(1.0 + jnp.exp(-jnp.abs(x)))
        decay = log_sig * (1.0 / gate_norm_term) + spikes[:, h : h + 1]
        high = decay.astype(BF16)
        rest = decay - high.astype(F32)
        mid = rest.astype(BF16)
        low = (rest - mid.astype(F32)).astype(BF16)
        cum = dot(tri, high) + dot(tri, mid) + dot(tri, low)
        cum_ref[:, cols] = cum
        total = cum[tok - 1 : tok, :]
        if h == 0:
            get_k.wait()
            get_v.wait()
        k_out = (k_ref[:, cols].astype(F32) * jnp.exp(total - cum)).astype(BF16)
        final = dot(k_out, v_ref[:, h * vd : (h + 1) * vd], TN).astype(BF16)
        rate = jnp.broadcast_to(jnp.exp(total), (8, kd))
        for r in range(per):
            for w in range(wide):
                send_ref[h * per + r, w * rows : (w + 1) * rows, :] = final[
                    r * rows : (r + 1) * rows, w * kd : (w + 1) * kd
                ]
            turned = pltpu.roll(rate, (kd - r * rows) % kd, 1) if r else rate
            coarse = turned.astype(BF16).astype(F32)
            send_ref[h * per + r, wide * rows : wide * rows + 8, :] = jnp.where(
                odd, turned - coarse, coarse
            ).astype(BF16)


def inside_kernel(
    who_ref, cum_ref, q_hbm, k_hbm, v_hbm, open_hbm, inside_ref, far_ref, open_ref, q_ref, k_ref, v_ref, sems
):
    mine = open_ref.shape[0]
    first = pl.multiple_of(who_ref[0] * mine, mine)
    for c in fetch(
        sems, (q_hbm, q_ref), (k_hbm, k_ref), (v_hbm, v_ref), (open_hbm.at[pl.ds(first, mine), :], open_ref)
    ):
        c.wait()
    tok, width = q_ref.shape
    kd = 128
    heads = width // kd
    vd = v_ref.shape[1] // heads
    scale = kd ** (-0.5)
    for h in range(heads):
        cols = slice(h * kd, (h + 1) * kd)
        vcols = slice(h * vd, (h + 1) * vd)
        for i in range(tok // BLOCK):
            lo, hi = i * BLOCK, (i + 1) * BLOCK
            q = q_ref[lo:hi, cols].astype(F32) * scale
            cum = cum_ref[lo:hi, cols]
            far_ref[lo:hi, cols] = (q * jnp.exp(cum)).astype(BF16)
            if i:
                base = cum_ref[lo - 1 : lo, cols]
                q_in = (q * jnp.exp(cum - base)).astype(BF16)
                k_in = (k_ref[0:hi, cols].astype(F32) * jnp.exp(base - cum_ref[0:hi, cols])).astype(BF16)
            else:
                q_in = (q * jnp.exp(cum)).astype(BF16)
                k_in = (k_ref[0:hi, cols].astype(F32) * jnp.exp(-cum)).astype(BF16)
            scores = dot(q_in, k_in, NT)
            seen = (
                lax.broadcasted_iota(jnp.int32, (BLOCK, hi), 0) + lo
                >= lax.broadcasted_iota(jnp.int32, (BLOCK, hi), 1)
            )
            scores = jnp.where(seen, scores, 0.0).astype(BF16)
            inside_ref[lo:hi, vcols] = dot(scores, v_ref[0:hi, vcols])


def chain_kernel(got_ref, open_ref, out_ref):
    group = got_ref.shape[0]
    rows, vd = open_ref.shape
    wide = vd // 128
    where = lax.broadcasted_iota(jnp.int32, (8, 128), 0)
    parts = []
    for g in range(group // 8):
        table = jnp.zeros((8, 128), F32)
        for d in range(8):
            pair = got_ref[g * 8 + d, wide * rows : wide * rows + 8, :].astype(F32)
            table = jnp.where(where == d, pair + pltpu.roll(pair, 1, 0), table)
        parts.append(table)
    rates = jnp.transpose(jnp.concatenate(parts, axis=0))
    states = [open_ref[:, w * 128 : (w + 1) * 128] for w in range(wide)]
    for d in range(group):
        rate = jnp.broadcast_to(rates[0:rows, d : d + 1], (rows, 128))
        for w in range(wide):
            out_ref[d, :, w * 128 : (w + 1) * 128] = states[w].astype(BF16)
            states[w] = rate * states[w] + got_ref[d, w * rows : (w + 1) * rows, :].astype(F32)


def project_kernel(who_ref, inside_ref, far_ref, start_ref, *refs):
    gain_hbm, mine, other, out_hbm = refs[0], refs[1:5], refs[5:9], refs[9]
    normed, weight, gain_ref, tiles, in_sems, out_sems = refs[10:]
    core, color = who_ref[1], who_ref[2]
    half = normed.shape[1] // 2
    piece = half // 4
    model = weight.shape[0]
    heads = 4
    kd, vd = far_ref.shape[1] // heads, start_ref.shape[1]
    halves = 2
    rows = model // halves
    pairs = [(gain_hbm, gain_ref)]
    for part in range(halves):
        span = pl.ds(part * rows, rows)
        for n in range(4):
            at = lax.rem(color + n, 4) * piece
            for base, src in ((core * half, mine[n]), ((1 - core) * half, other[n])):
                to = pl.ds(pl.multiple_of(base + at, piece), piece)
                pairs.append((src.at[span, :], weight.at[span, to]))
    copies = fetch(in_sems, *pairs)
    copies[0].wait()
    for h in range(heads):
        o = inside_ref[:, h * vd : (h + 1) * vd] + dot(
            far_ref[:, h * kd : (h + 1) * kd], start_ref[h * kd : (h + 1) * kd, :]
        )
        spread = lax.rsqrt(jnp.mean(o * o, axis=-1, keepdims=True) + norm_eps)
        normed[:, h * vd : (h + 1) * vd] = (o * spread * gain_ref[...]).astype(BF16)
    tile = model // TILES
    outs = []
    for t in range(TILES):
        if t % (TILES // halves) == 0:
            part = t // (TILES // halves)
            for c in copies[1 + 8 * part : 9 + 8 * part]:
                c.wait()
        tiles[t] = dot(normed[...], weight[t * tile : (t + 1) * tile, :], NT).astype(BF16)
        c = pltpu.make_async_copy(tiles.at[t], out_hbm.at[:, pl.ds(t * tile, tile)], out_sems.at[t])
        c.start()
        outs.append(c)
    for c in outs:
        c.wait()


def hbm(*arrays):
    return [pltpu.with_memory_space_constraint(a, pltpu.HBM) for a in arrays]


def vmem(*arrays):
    return [pltpu.with_memory_space_constraint(a, pltpu.VMEM) for a in arrays]


def params(mib):
    return pltpu.CompilerParams(vmem_limit_bytes=mib * 2**20)


def cost(flops):
    return pl.CostEstimate(flops=flops, bytes_accessed=10**6, transcendentals=0)


def on_device(
    queries,
    head_keys,
    decay_preact,
    values,
    extra_log_decay,
    decay_offset_bias,
    opening_state,
    output_norm_gain,
    output_weight,
):
    tok, seqs, width = queries.shape
    heads, kd = decay_offset_bias.shape
    vd = output_norm_gain.shape[0]
    group = lax.axis_size("sp")
    plane = lax.axis_size("dp")
    share = output_weight.shape[1]
    model = share * plane
    piece = heads * vd // 8
    rows = heads * kd // group
    packed = rows * vd // 128 + 8
    sp, dp = lax.axis_index("sp"), lax.axis_index("dp")
    z, y = lax.div(dp, SIDE), lax.rem(dp, SIDE)
    who = jnp.stack([sp, lax.rem(sp, 2), lax.rem(y + 2 * z, 4), z]).astype(jnp.int32)
    dma = pltpu.SemaphoreType.DMA

    q = queries.reshape(tok, width)
    k = head_keys.reshape(tok, width)
    x = decay_preact.reshape(tok, width)
    v = values.reshape(tok, heads * vd)
    opening = opening_state.reshape(heads * kd, vd)

    def from_offset(dz, dy):
        return [
            (((i + dz) % SIDE) * SIDE + (j + dy) % SIDE, i * SIDE + j)
            for i in range(plane // SIDE)
            for j in range(SIDE)
        ]

    spread = pl.pallas_call(
        spread_kernel,
        out_shape=pltpu.VMEM((plane, share, piece), BF16),
        in_specs=[SMEM, HBM],
        out_specs=VMEM,
        scratch_shapes=[pltpu.VMEM((4, share, piece), BF16), dma((4,))],
        compiler_params=params(4),
        cost_estimate=cost(10**6),
        name="spread",
    )(who, *hbm(output_weight.T))
    eighth = lax.all_to_all(spread, "dp", 0, 0, tiled=True).reshape(model, piece)
    mine = [eighth]
    for o in ((0, 1), (1, 0), (0, -1)):
        mine.append(lax.ppermute(eighth, "dp", from_offset(*o)))
    other = []
    for chunk in mine:
        other.append(lax.ppermute(chunk, "sp", [(i, i ^ 1) for i in range(group)]))

    send, cum = pl.pallas_call(
        summary_kernel,
        out_shape=(
            pltpu.VMEM((group, packed, 128), BF16),
            pltpu.VMEM((tok, width), F32),
        ),
        in_specs=[HBM] * 5,
        out_specs=(VMEM, VMEM),
        scratch_shapes=[
            pltpu.VMEM((tok, width), BF16),
            pltpu.VMEM((tok, width), BF16),
            pltpu.VMEM((tok, heads * vd), BF16),
            pltpu.VMEM(extra_log_decay.shape, F32),
            pltpu.VMEM((heads, kd), F32),
            dma((5,)),
        ],
        compiler_params=params(16),
        cost_estimate=cost(3 * 10**8),
        name="summary",
    )(*hbm(k, x, v, extra_log_decay, decay_offset_bias))

    got = lax.all_to_all(send, "sp", 0, 0, tiled=True)

    inside, far, own_opening = pl.pallas_call(
        inside_kernel,
        out_shape=(
            pltpu.VMEM((tok, heads * vd), F32),
            pltpu.VMEM((tok, width), BF16),
            pltpu.VMEM((rows, vd), F32),
        ),
        in_specs=[SMEM, VMEM] + [HBM] * 4,
        out_specs=(VMEM, VMEM, VMEM),
        scratch_shapes=[
            pltpu.VMEM((tok, width), BF16),
            pltpu.VMEM((tok, width), BF16),
            pltpu.VMEM((tok, heads * vd), BF16),
            dma((4,)),
        ],
        compiler_params=params(16),
        cost_estimate=cost(3 * 10**8),
        name="inside",
    )(who, *vmem(cum), *hbm(q, k, v, opening))

    starts = pl.pallas_call(
        chain_kernel,
        out_shape=pltpu.VMEM((group, rows, vd), BF16),
        in_specs=[VMEM, VMEM],
        out_specs=VMEM,
        compiler_params=params(8),
        cost_estimate=cost(10**7),
        name="chain",
    )(*vmem(got, own_opening))

    start = lax.all_to_all(starts, "sp", 0, 0, tiled=True).reshape(heads * kd, vd)

    out = pl.pallas_call(
        project_kernel,
        out_shape=jax.ShapeDtypeStruct((tok, model), BF16),
        in_specs=[SMEM] + [VMEM] * 3 + [HBM] * 9,
        out_specs=HBM,
        scratch_shapes=[
            pltpu.VMEM((tok, heads * vd), BF16),
            pltpu.VMEM((model, heads * vd), BF16),
            pltpu.VMEM((1, vd), F32),
            pltpu.VMEM((TILES, tok, model // TILES), BF16),
            dma((17,)),
            dma((TILES,)),
        ],
        compiler_params=params(24),
        cost_estimate=cost(10**9),
        name="project",
    )(who, *vmem(inside, far, start), *hbm(output_norm_gain.reshape(1, vd), *mine, *other))
    return out.reshape(tok, seqs, model)


def solution(mesh):
    return jax.shard_map(
        on_device,
        mesh=mesh,
        in_specs=(
            P("sp", "dp", None),
            P("sp", "dp", None),
            P("sp", "dp", None),
            P("sp", "dp", None),
            P("dp", "sp"),
            P(),
            P("dp", None, None, None),
            P(),
            P(None, "dp"),
        ),
        out_specs=P("sp", "dp", None),
        check_vma=False,
    )
```

```python
import jax
import jax.numpy as jnp
from jax import lax
from jax.experimental import pallas as pl
from jax.experimental.pallas import tpu as pltpu
from jax.sharding import PartitionSpec as P


BLOCK = 64
gate_norm_term = 16.0
norm_eps = 1e-05
F32 = jnp.float32
BF16 = jnp.bfloat16
VMEM = pl.BlockSpec(memory_space=pltpu.VMEM)
HBM = pl.BlockSpec(memory_space=pltpu.HBM)
SMEM = pl.BlockSpec(memory_space=pltpu.SMEM)
SIDE = 8
TILES = 4


def dot(a, b, dims=(((1,), (0,)), ((), ()))):
    return lax.dot_general(a, b, dims, preferred_element_type=F32)


NT = (((1,), (1,)), ((), ()))
TN = (((0,), (0,)), ((), ()))


def two_parts(rate):
    coarse = rate.astype(BF16).astype(F32)
    odd = lax.broadcasted_iota(jnp.int32, rate.shape, 0) % 2 == 1
    return jnp.where(odd, rate - coarse, coarse).astype(BF16)


def rate_table(pieces):
    where = lax.broadcasted_iota(jnp.int32, (8, 128), 0)
    table = jnp.zeros((8, 128), F32)
    for d, piece in enumerate(pieces):
        pair = piece.astype(F32)
        table = jnp.where(where == d, pair + pltpu.roll(pair, 1, 0), table)
    return table


def combine_kernel(who_ref, own_ref, other_ref, send_ref):
    core = who_ref[1]
    chips, packed, lanes = send_ref.shape
    data = packed - 8
    rows = data // 2
    own = own_ref[pl.ds(core * chips, chips)]
    other = other_ref[pl.ds(core * chips, chips)]
    early = jnp.where(core == 0, own.astype(F32), other.astype(F32))
    late = jnp.where(core == 0, other.astype(F32), own.astype(F32))
    late_rates = rate_table([late[n, data:] for n in range(chips)])
    rates = late_rates * rate_table([early[n, data:] for n in range(chips)])
    turned = jnp.transpose(late_rates)
    for n in range(chips):
        rate = jnp.broadcast_to(turned[0:rows, n : n + 1], (rows, lanes))
        for w in range(2):
            at = slice(w * rows, (w + 1) * rows)
            send_ref[n, at, :] = (rate * early[n, at] + late[n, at]).astype(BF16)
        send_ref[n, data:, :] = two_parts(jnp.broadcast_to(rates[n : n + 1, :], (8, lanes)))


def fetch(sems, *pairs):
    copies = [pltpu.make_async_copy(a, b, sems.at[n]) for n, (a, b) in enumerate(pairs)]
    for c in copies:
        c.start()
    return copies


def spread_kernel(who_ref, weight_hbm, out_ref, quarters, sems):
    core = who_ref[1]
    width = out_ref.shape[2]
    pairs = []
    for c in range(4):
        first = pl.multiple_of((core * 4 + c) * width, width)
        pairs.append((weight_hbm.at[:, pl.ds(first, width)], quarters.at[c]))
    for c in fetch(sems, *pairs):
        c.wait()
    for d in range(out_ref.shape[0]):
        out_ref[d] = quarters[(d % SIDE + 2 * (d // SIDE)) % 4]


def summary_kernel(k_hbm, x_hbm, v_hbm, extra_hbm, bias_hbm, send_ref, cum_ref, k_ref, x_ref, v_ref, extra_ref, bias_ref, sems):
    get_x, get_extra, get_bias, get_k, get_v = fetch(
        sems, (x_hbm, x_ref), (extra_hbm, extra_ref), (bias_hbm, bias_ref), (k_hbm, k_ref), (v_hbm, v_ref)
    )
    tok = k_ref.shape[0]
    heads, kd = bias_ref.shape
    vd = v_ref.shape[1] // heads
    group = send_ref.shape[0] - 1
    per, rows = group // heads, kd * heads // group
    wide = vd // kd
    tri = (
        lax.broadcasted_iota(jnp.int32, (tok, tok), 0)
        >= lax.broadcasted_iota(jnp.int32, (tok, tok), 1)
    ).astype(BF16)
    get_extra.wait()
    spikes = jnp.transpose(extra_ref[...])
    get_bias.wait()
    get_x.wait()
    for h in range(heads):
        cols = slice(h * kd, (h + 1) * kd)
        x = x_ref[:, cols].astype(F32) + bias_ref[h : h + 1, :]
        log_sig = jnp.minimum(x, 0.0) - jnp.log(1.0 + jnp.exp(-jnp.abs(x)))
        decay = log_sig * (1.0 / gate_norm_term) + spikes[:, h : h + 1]
        high = decay.astype(BF16)
        rest = decay - high.astype(F32)
        mid = rest.astype(BF16)
        low = (rest - mid.astype(F32)).astype(BF16)
        cum = dot(tri, high) + dot(tri, mid) + dot(tri, low)
        cum_ref[:, cols] = cum
        total = cum[tok - 1 : tok, :]
        if h == 0:
            get_k.wait()
            get_v.wait()
        k_out = (k_ref[:, cols].astype(F32) * jnp.exp(total - cum)).astype(BF16)
        final = dot(k_out, v_ref[:, h * vd : (h + 1) * vd], TN).astype(BF16)
        rate = jnp.broadcast_to(jnp.exp(total), (8, kd))
        send_ref[group, 16 * h : 16 * h + 8, :] = two_parts(rate)
        for r in range(per):
            for w in range(wide):
                send_ref[h * per + r, w * rows : (w + 1) * rows, :] = final[
                    r * rows : (r + 1) * rows, w * kd : (w + 1) * kd
                ]
            turned = pltpu.roll(rate, (kd - r * rows) % kd, 1) if r else rate
            send_ref[h * per + r, wide * rows : wide * rows + 8, :] = two_parts(turned)


def inside_kernel(
    who_ref, cum_ref, other_ref, q_hbm, k_hbm, v_hbm, open_hbm, inside_ref, far_ref, open_ref, q_ref, k_ref, v_ref, sems
):
    mine = open_ref.shape[0]
    second = who_ref[1] == 1
    group = other_ref.shape[0] - 1
    first = pl.multiple_of(who_ref[0] * mine, mine)
    for c in fetch(
        sems, (q_hbm, q_ref), (k_hbm, k_ref), (v_hbm, v_ref), (open_hbm.at[pl.ds(first, mine), :], open_ref)
    ):
        c.wait()
    tok, width = q_ref.shape
    kd = 128
    heads = width // kd
    vd = v_ref.shape[1] // heads
    scale = kd ** (-0.5)
    for h in range(heads):
        cols = slice(h * kd, (h + 1) * kd)
        vcols = slice(h * vd, (h + 1) * vd)
        pair = other_ref[group, 16 * h : 16 * h + 8, :].astype(F32)
        rate = jnp.where(second, pair[0:1, :] + pair[1:2, :], 1.0)
        blocks = range(group * h // heads, group * (h + 1) // heads)
        before = jnp.concatenate(
            [
                jnp.concatenate([other_ref[b, w * mine : (w + 1) * mine, :] for b in blocks], axis=0)
                for w in range(vd // kd)
            ],
            axis=1,
        )
        before = jnp.where(second, before.astype(F32), 0.0).astype(BF16)
        for i in range(tok // BLOCK):
            lo, hi = i * BLOCK, (i + 1) * BLOCK
            q = q_ref[lo:hi, cols].astype(F32) * scale
            cum = cum_ref[lo:hi, cols]
            far = q * jnp.exp(cum)
            far_ref[lo:hi, cols] = (far * rate).astype(BF16)
            if i:
                base = cum_ref[lo - 1 : lo, cols]
                q_in = (q * jnp.exp(cum - base)).astype(BF16)
                k_in = (k_ref[0:hi, cols].astype(F32) * jnp.exp(base - cum_ref[0:hi, cols])).astype(BF16)
            else:
                q_in = (q * jnp.exp(cum)).astype(BF16)
                k_in = (k_ref[0:hi, cols].astype(F32) * jnp.exp(-cum)).astype(BF16)
            scores = dot(q_in, k_in, NT)
            seen = (
                lax.broadcasted_iota(jnp.int32, (BLOCK, hi), 0) + lo
                >= lax.broadcasted_iota(jnp.int32, (BLOCK, hi), 1)
            )
            scores = jnp.where(seen, scores, 0.0).astype(BF16)
            inside_ref[lo:hi, vcols] = dot(scores, v_ref[0:hi, vcols]) + dot(far.astype(BF16), before)


def chain_kernel(got_ref, open_ref, out_ref):
    chips, packed, lanes = got_ref.shape
    rows, vd = open_ref.shape
    wide = vd // lanes
    rates = jnp.transpose(rate_table([got_ref[d, packed - 8 :, :] for d in range(chips)]))
    states = [open_ref[:, w * lanes : (w + 1) * lanes] for w in range(wide)]
    for d in range(chips):
        rate = jnp.broadcast_to(rates[0:rows, d : d + 1], (rows, lanes))
        for w in range(wide):
            rounded = states[w].astype(BF16)
            for c in range(2):
                out_ref[2 * d + c, :, w * lanes : (w + 1) * lanes] = rounded
            states[w] = rate * states[w] + got_ref[d, w * rows : (w + 1) * rows, :].astype(F32)


def project_kernel(who_ref, inside_ref, far_ref, start_ref, *refs):
    gain_hbm, mine, other, out_hbm = refs[0], refs[1:5], refs[5:9], refs[9]
    normed, weight, gain_ref, tiles, in_sems, out_sems = refs[10:]
    core, color = who_ref[1], who_ref[2]
    half = normed.shape[1] // 2
    piece = half // 4
    model = weight.shape[0]
    heads = 4
    kd, vd = far_ref.shape[1] // heads, start_ref.shape[2]
    group = start_ref.shape[0]
    halves = 2
    rows = model // halves
    pairs = [(gain_hbm, gain_ref)]
    for part in range(halves):
        span = pl.ds(part * rows, rows)
        for n in range(4):
            at = lax.rem(color + n, 4) * piece
            for base, src in ((core * half, mine[n]), ((1 - core) * half, other[n])):
                to = pl.ds(pl.multiple_of(base + at, piece), piece)
                pairs.append((src.at[span, :], weight.at[span, to]))
    copies = fetch(in_sems, *pairs)
    copies[0].wait()
    for h in range(heads):
        blocks = range(group * h // heads, group * (h + 1) // heads)
        start = jnp.concatenate([start_ref[2 * (b % SIDE) + b // SIDE] for b in blocks], axis=0)
        o = inside_ref[:, h * vd : (h + 1) * vd] + dot(far_ref[:, h * kd : (h + 1) * kd], start)
        spread = lax.rsqrt(jnp.mean(o * o, axis=-1, keepdims=True) + norm_eps)
        normed[:, h * vd : (h + 1) * vd] = (o * spread * gain_ref[...]).astype(BF16)
    tile = model // TILES
    outs = []
    for t in range(TILES):
        if t % (TILES // halves) == 0:
            part = t // (TILES // halves)
            for c in copies[1 + 8 * part : 9 + 8 * part]:
                c.wait()
        tiles[t] = dot(normed[...], weight[t * tile : (t + 1) * tile, :], NT).astype(BF16)
        c = pltpu.make_async_copy(tiles.at[t], out_hbm.at[:, pl.ds(t * tile, tile)], out_sems.at[t])
        c.start()
        outs.append(c)
    for c in outs:
        c.wait()


def hbm(*arrays):
    return [pltpu.with_memory_space_constraint(a, pltpu.HBM) for a in arrays]


def vmem(*arrays):
    return [pltpu.with_memory_space_constraint(a, pltpu.VMEM) for a in arrays]


def params(mib):
    return pltpu.CompilerParams(vmem_limit_bytes=mib * 2**20)


def cost(flops):
    return pl.CostEstimate(flops=flops, bytes_accessed=10**6, transcendentals=0)


def on_device(
    queries,
    head_keys,
    decay_preact,
    values,
    extra_log_decay,
    decay_offset_bias,
    opening_state,
    output_norm_gain,
    output_weight,
):
    tok, seqs, width = queries.shape
    heads, kd = decay_offset_bias.shape
    vd = output_norm_gain.shape[0]
    group = lax.axis_size("sp")
    plane = lax.axis_size("dp")
    share = output_weight.shape[1]
    model = share * plane
    piece = heads * vd // 8
    rows = heads * kd // group
    packed = rows * vd // 128 + 8
    sp, dp = lax.axis_index("sp"), lax.axis_index("dp")
    z, y = lax.div(dp, SIDE), lax.rem(dp, SIDE)
    chip, core = lax.div(sp, 2), lax.rem(sp, 2)
    block = core * (group // 2) + chip
    who = jnp.stack([block, core, lax.rem(y + 2 * z, 4)]).astype(jnp.int32)
    dma = pltpu.SemaphoreType.DMA

    q = queries.reshape(tok, width)
    k = head_keys.reshape(tok, width)
    x = decay_preact.reshape(tok, width)
    v = values.reshape(tok, heads * vd)
    opening = opening_state.reshape(heads * kd, vd)

    def from_offset(dz, dy):
        return [
            (((i + dz) % SIDE) * SIDE + (j + dy) % SIDE, i * SIDE + j)
            for i in range(plane // SIDE)
            for j in range(SIDE)
        ]

    spread = pl.pallas_call(
        spread_kernel,
        out_shape=pltpu.VMEM((plane, share, piece), BF16),
        in_specs=[SMEM, HBM],
        out_specs=VMEM,
        scratch_shapes=[pltpu.VMEM((4, share, piece), BF16), dma((4,))],
        compiler_params=params(4),
        cost_estimate=cost(10**6),
        name="spread",
    )(who, *hbm(output_weight.T))
    eighth = lax.all_to_all(spread, "dp", 0, 0, tiled=True).reshape(model, piece)
    mine = [eighth]
    for o in ((0, 1), (1, 0), (0, -1)):
        mine.append(lax.ppermute(eighth, "dp", from_offset(*o)))
    other = []
    for chunk in mine:
        other.append(lax.ppermute(chunk, "sp", [(i, i ^ 1) for i in range(group)]))

    final, cum = pl.pallas_call(
        summary_kernel,
        out_shape=(
            pltpu.VMEM((group + 1, packed, 128), BF16),
            pltpu.VMEM((tok, width), F32),
        ),
        in_specs=[HBM] * 5,
        out_specs=(VMEM, VMEM),
        scratch_shapes=[
            pltpu.VMEM((tok, width), BF16),
            pltpu.VMEM((tok, width), BF16),
            pltpu.VMEM((tok, heads * vd), BF16),
            pltpu.VMEM(extra_log_decay.shape, F32),
            pltpu.VMEM((heads, kd), F32),
            dma((5,)),
        ],
        compiler_params=params(16),
        cost_estimate=cost(3 * 10**8),
        name="summary",
    )(*hbm(k, x, v, extra_log_decay, decay_offset_bias))

    other_final = lax.ppermute(final, "sp", [(i, i ^ 1) for i in range(group)])
    send = pl.pallas_call(
        combine_kernel,
        out_shape=pltpu.VMEM((group // 2, packed, 128), BF16),
        in_specs=[SMEM, VMEM, VMEM],
        out_specs=VMEM,
        compiler_params=params(8),
        cost_estimate=cost(10**7),
        name="combine",
    )(who, *vmem(final, other_final))
    chips = [[2 * i + c for i in range(group // 2)] for c in range(2)]
    got = lax.all_to_all(send, "sp", 0, 0, axis_index_groups=chips, tiled=True)

    inside, far, own_opening = pl.pallas_call(
        inside_kernel,
        out_shape=(
            pltpu.VMEM((tok, heads * vd), F32),
            pltpu.VMEM((tok, width), BF16),
            pltpu.VMEM((rows, vd), F32),
        ),
        in_specs=[SMEM, VMEM, VMEM] + [HBM] * 4,
        out_specs=(VMEM, VMEM, VMEM),
        scratch_shapes=[
            pltpu.VMEM((tok, width), BF16),
            pltpu.VMEM((tok, width), BF16),
            pltpu.VMEM((tok, heads * vd), BF16),
            dma((4,)),
        ],
        compiler_params=params(16),
        cost_estimate=cost(3 * 10**8),
        name="inside",
    )(who, *vmem(cum, other_final), *hbm(q, k, v, opening))

    starts = pl.pallas_call(
        chain_kernel,
        out_shape=pltpu.VMEM((group, rows, vd), BF16),
        in_specs=[VMEM, VMEM],
        out_specs=VMEM,
        compiler_params=params(8),
        cost_estimate=cost(10**7),
        name="chain",
    )(*vmem(got, own_opening))

    start = lax.all_to_all(starts, "sp", 0, 0, tiled=True)

    out = pl.pallas_call(
        project_kernel,
        out_shape=jax.ShapeDtypeStruct((tok, model), BF16),
        in_specs=[SMEM] + [VMEM] * 3 + [HBM] * 9,
        out_specs=HBM,
        scratch_shapes=[
            pltpu.VMEM((tok, heads * vd), BF16),
            pltpu.VMEM((model, heads * vd), BF16),
            pltpu.VMEM((1, vd), F32),
            pltpu.VMEM((TILES, tok, model // TILES), BF16),
            dma((17,)),
            dma((TILES,)),
        ],
        compiler_params=params(24),
        cost_estimate=cost(10**9),
        name="project",
    )(who, *vmem(inside, far, start), *hbm(output_norm_gain.reshape(1, vd), *mine, *other))
    return out.reshape(tok, seqs, model)


def solution(mesh):
    return jax.shard_map(
        on_device,
        mesh=mesh,
        in_specs=(
            P("sp", "dp", None),
            P("sp", "dp", None),
            P("sp", "dp", None),
            P("sp", "dp", None),
            P("dp", "sp"),
            P(),
            P("dp", None, None, None),
            P(),
            P(None, "dp"),
        ),
        out_specs=P("sp", "dp", None),
        check_vma=False,
    )
```

```python
import jax
import jax.numpy as jnp
from jax import lax
from jax.experimental import pallas as pl
from jax.experimental.pallas import tpu as pltpu
from jax.sharding import PartitionSpec as P


BLOCK = 64
gate_norm_term = 16.0
norm_eps = 1e-05
F32 = jnp.float32
BF16 = jnp.bfloat16
VMEM = pl.BlockSpec(memory_space=pltpu.VMEM)
HBM = pl.BlockSpec(memory_space=pltpu.HBM)
SMEM = pl.BlockSpec(memory_space=pltpu.SMEM)
SIDE = 8
TILES = 4


def dot(a, b, dims=(((1,), (0,)), ((), ()))):
    return lax.dot_general(a, b, dims, preferred_element_type=F32)


NT = (((1,), (1,)), ((), ()))
TN = (((0,), (0,)), ((), ()))


def two_parts(rate):
    coarse = rate.astype(BF16).astype(F32)
    odd = lax.broadcasted_iota(jnp.int32, rate.shape, 0) % 2 == 1
    return jnp.where(odd, rate - coarse, coarse).astype(BF16)


def rate_table(pieces):
    where = lax.broadcasted_iota(jnp.int32, (8, 128), 0)
    table = jnp.zeros((8, 128), F32)
    for d, piece in enumerate(pieces):
        pair = piece.astype(F32)
        table = jnp.where(where == d, pair + pltpu.roll(pair, 1, 0), table)
    return table


def combine_kernel(who_ref, own_ref, other_ref, send_ref):
    core = who_ref[1]
    chips, packed, lanes = send_ref.shape
    data = packed - 8
    rows = data // 2
    own = own_ref[pl.ds(core * chips, chips)]
    other = other_ref[pl.ds(core * chips, chips)]
    early = jnp.where(core == 0, own.astype(F32), other.astype(F32))
    late = jnp.where(core == 0, other.astype(F32), own.astype(F32))
    late_rates = rate_table([late[n, data:] for n in range(chips)])
    rates = late_rates * rate_table([early[n, data:] for n in range(chips)])
    turned = jnp.transpose(late_rates)
    for n in range(chips):
        rate = jnp.broadcast_to(turned[0:rows, n : n + 1], (rows, lanes))
        for w in range(2):
            at = slice(w * rows, (w + 1) * rows)
            send_ref[n, at, :] = (rate * early[n, at] + late[n, at]).astype(BF16)
        send_ref[n, data:, :] = two_parts(jnp.broadcast_to(rates[n : n + 1, :], (8, lanes)))


def fetch(sems, *pairs):
    copies = [pltpu.make_async_copy(a, b, sems.at[n]) for n, (a, b) in enumerate(pairs)]
    for c in copies:
        c.start()
    return copies


def spread_kernel(who_ref, weight_hbm, out_hbm, quarters, pattern, sems, out_sems):
    core = who_ref[1]
    width = quarters.shape[2]
    pairs = []
    for c in range(4):
        first = pl.multiple_of((core * 4 + c) * width, width)
        pairs.append((weight_hbm.at[:, pl.ds(first, width)], quarters.at[c]))
    for c in fetch(sems, *pairs):
        c.wait()
    period = pattern.shape[0]
    for d in range(period):
        pattern[d] = quarters[(d % SIDE + 2 * (d // SIDE)) % 4]
    spans = range(0, out_hbm.shape[0], period)
    for c in fetch(out_sems, *[(pattern, out_hbm.at[pl.ds(d, period)]) for d in spans]):
        c.wait()


def summary_kernel(k_hbm, x_hbm, v_hbm, extra_hbm, bias_hbm, send_ref, cum_ref, k_ref, x_ref, v_ref, extra_ref, bias_ref, sems):
    get_x, get_extra, get_bias, get_k, get_v = fetch(
        sems, (x_hbm, x_ref), (extra_hbm, extra_ref), (bias_hbm, bias_ref), (k_hbm, k_ref), (v_hbm, v_ref)
    )
    tok = k_ref.shape[0]
    heads, kd = bias_ref.shape
    vd = v_ref.shape[1] // heads
    group = send_ref.shape[0] - 1
    per, rows = group // heads, kd * heads // group
    wide = vd // kd
    tri = (
        lax.broadcasted_iota(jnp.int32, (tok, tok), 0)
        >= lax.broadcasted_iota(jnp.int32, (tok, tok), 1)
    ).astype(BF16)
    get_extra.wait()
    spikes = jnp.transpose(extra_ref[...])
    get_bias.wait()
    get_x.wait()
    for h in range(heads):
        cols = slice(h * kd, (h + 1) * kd)
        x = x_ref[:, cols].astype(F32) + bias_ref[h : h + 1, :]
        log_sig = jnp.minimum(x, 0.0) - jnp.log(1.0 + jnp.exp(-jnp.abs(x)))
        decay = log_sig * (1.0 / gate_norm_term) + spikes[:, h : h + 1]
        high = decay.astype(BF16)
        rest = decay - high.astype(F32)
        mid = rest.astype(BF16)
        low = (rest - mid.astype(F32)).astype(BF16)
        cum = dot(tri, high) + dot(tri, mid) + dot(tri, low)
        cum_ref[:, cols] = cum
        total = cum[tok - 1 : tok, :]
        if h == 0:
            get_k.wait()
            get_v.wait()
        k_out = (k_ref[:, cols].astype(F32) * jnp.exp(total - cum)).astype(BF16)
        final = dot(k_out, v_ref[:, h * vd : (h + 1) * vd], TN).astype(BF16)
        rate = jnp.broadcast_to(jnp.exp(total), (8, kd))
        send_ref[group, 16 * h : 16 * h + 8, :] = two_parts(rate)
        for r in range(per):
            for w in range(wide):
                send_ref[h * per + r, w * rows : (w + 1) * rows, :] = final[
                    r * rows : (r + 1) * rows, w * kd : (w + 1) * kd
                ]
            turned = pltpu.roll(rate, (kd - r * rows) % kd, 1) if r else rate
            send_ref[h * per + r, wide * rows : wide * rows + 8, :] = two_parts(turned)


def inside_kernel(
    who_ref, cum_ref, other_ref, q_hbm, k_hbm, v_hbm, open_hbm, inside_ref, far_ref, open_ref, q_ref, k_ref, v_ref, sems
):
    mine = open_ref.shape[0]
    second = who_ref[1] == 1
    group = other_ref.shape[0] - 1
    first = pl.multiple_of(who_ref[0] * mine, mine)
    for c in fetch(
        sems, (q_hbm, q_ref), (k_hbm, k_ref), (v_hbm, v_ref), (open_hbm.at[pl.ds(first, mine), :], open_ref)
    ):
        c.wait()
    tok, width = q_ref.shape
    kd = 128
    heads = width // kd
    vd = v_ref.shape[1] // heads
    scale = kd ** (-0.5)
    for h in range(heads):
        cols = slice(h * kd, (h + 1) * kd)
        vcols = slice(h * vd, (h + 1) * vd)
        pair = other_ref[group, 16 * h : 16 * h + 8, :].astype(F32)
        rate = jnp.where(second, pair[0:1, :] + pair[1:2, :], 1.0)
        blocks = range(group * h // heads, group * (h + 1) // heads)
        before = jnp.concatenate(
            [
                jnp.concatenate([other_ref[b, w * mine : (w + 1) * mine, :] for b in blocks], axis=0)
                for w in range(vd // kd)
            ],
            axis=1,
        )
        before = jnp.where(second, before.astype(F32), 0.0).astype(BF16)
        for i in range(tok // BLOCK):
            lo, hi = i * BLOCK, (i + 1) * BLOCK
            q = q_ref[lo:hi, cols].astype(F32) * scale
            cum = cum_ref[lo:hi, cols]
            far = q * jnp.exp(cum)
            far_ref[lo:hi, cols] = (far * rate).astype(BF16)
            if i:
                base = cum_ref[lo - 1 : lo, cols]
                q_in = (q * jnp.exp(cum - base)).astype(BF16)
                k_in = (k_ref[0:hi, cols].astype(F32) * jnp.exp(base - cum_ref[0:hi, cols])).astype(BF16)
            else:
                q_in = (q * jnp.exp(cum)).astype(BF16)
                k_in = (k_ref[0:hi, cols].astype(F32) * jnp.exp(-cum)).astype(BF16)
            scores = dot(q_in, k_in, NT)
            seen = (
                lax.broadcasted_iota(jnp.int32, (BLOCK, hi), 0) + lo
                >= lax.broadcasted_iota(jnp.int32, (BLOCK, hi), 1)
            )
            scores = jnp.where(seen, scores, 0.0).astype(BF16)
            inside_ref[lo:hi, vcols] = dot(scores, v_ref[0:hi, vcols]) + dot(far.astype(BF16), before)


def chain_kernel(got_ref, open_ref, out_ref):
    chips, packed, lanes = got_ref.shape
    rows, vd = open_ref.shape
    wide = vd // lanes
    rates = jnp.transpose(rate_table([got_ref[d, packed - 8 :, :] for d in range(chips)]))
    states = [open_ref[:, w * lanes : (w + 1) * lanes] for w in range(wide)]
    for d in range(chips):
        rate = jnp.broadcast_to(rates[0:rows, d : d + 1], (rows, lanes))
        for w in range(wide):
            rounded = states[w].astype(BF16)
            for c in range(2):
                out_ref[2 * d + c, :, w * lanes : (w + 1) * lanes] = rounded
            states[w] = rate * states[w] + got_ref[d, w * rows : (w + 1) * rows, :].astype(F32)


def project_kernel(who_ref, inside_ref, far_ref, start_ref, *refs):
    gain_hbm, mine, other, out_hbm = refs[0], refs[1:5], refs[5:9], refs[9]
    normed, weight, gain_ref, tiles, in_sems, out_sems = refs[10:]
    core, color = who_ref[1], who_ref[2]
    half = normed.shape[1] // 2
    piece = half // 4
    model = weight.shape[0]
    heads = 4
    kd, vd = far_ref.shape[1] // heads, start_ref.shape[2]
    group = start_ref.shape[0]
    halves = 2
    rows = model // halves
    pairs = [(gain_hbm, gain_ref)]
    for part in range(halves):
        span = pl.ds(part * rows, rows)
        for n in range(4):
            at = lax.rem(color + n, 4) * piece
            for base, src in ((core * half, mine[n]), ((1 - core) * half, other[n])):
                to = pl.ds(pl.multiple_of(base + at, piece), piece)
                pairs.append((src.at[span, :], weight.at[span, to]))
    copies = fetch(in_sems, *pairs)
    copies[0].wait()
    for h in range(heads):
        blocks = range(group * h // heads, group * (h + 1) // heads)
        start = jnp.concatenate([start_ref[2 * (b % SIDE) + b // SIDE] for b in blocks], axis=0)
        o = inside_ref[:, h * vd : (h + 1) * vd] + dot(far_ref[:, h * kd : (h + 1) * kd], start)
        spread = lax.rsqrt(jnp.mean(o * o, axis=-1, keepdims=True) + norm_eps)
        normed[:, h * vd : (h + 1) * vd] = (o * spread * gain_ref[...]).astype(BF16)
    tile = model // TILES
    outs = []
    for t in range(TILES):
        if t % (TILES // halves) == 0:
            part = t // (TILES // halves)
            for c in copies[1 + 8 * part : 9 + 8 * part]:
                c.wait()
        tiles[t] = dot(normed[...], weight[t * tile : (t + 1) * tile, :], NT).astype(BF16)
        c = pltpu.make_async_copy(tiles.at[t], out_hbm.at[:, pl.ds(t * tile, tile)], out_sems.at[t])
        c.start()
        outs.append(c)
    for c in outs:
        c.wait()


def hbm(*arrays):
    return [pltpu.with_memory_space_constraint(a, pltpu.HBM) for a in arrays]


def vmem(*arrays):
    return [pltpu.with_memory_space_constraint(a, pltpu.VMEM) for a in arrays]


def params(mib):
    return pltpu.CompilerParams(vmem_limit_bytes=mib * 2**20)


def cost(flops):
    return pl.CostEstimate(flops=flops, bytes_accessed=10**6, transcendentals=0)


def on_device(
    queries,
    head_keys,
    decay_preact,
    values,
    extra_log_decay,
    decay_offset_bias,
    opening_state,
    output_norm_gain,
    output_weight,
):
    tok, seqs, width = queries.shape
    heads, kd = decay_offset_bias.shape
    vd = output_norm_gain.shape[0]
    group = lax.axis_size("sp")
    plane = lax.axis_size("dp")
    share = output_weight.shape[1]
    model = share * plane
    piece = heads * vd // 8
    rows = heads * kd // group
    packed = rows * vd // 128 + 8
    sp, dp = lax.axis_index("sp"), lax.axis_index("dp")
    z, y = lax.div(dp, SIDE), lax.rem(dp, SIDE)
    chip, core = lax.div(sp, 2), lax.rem(sp, 2)
    block = core * (group // 2) + chip
    who = jnp.stack([block, core, lax.rem(y + 2 * z, 4)]).astype(jnp.int32)
    dma = pltpu.SemaphoreType.DMA

    q = queries.reshape(tok, width)
    k = head_keys.reshape(tok, width)
    x = decay_preact.reshape(tok, width)
    v = values.reshape(tok, heads * vd)
    opening = opening_state.reshape(heads * kd, vd)

    def from_offset(dz, dy):
        return [
            (((i + dz) % SIDE) * SIDE + (j + dy) % SIDE, i * SIDE + j)
            for i in range(plane // SIDE)
            for j in range(SIDE)
        ]

    spread = pl.pallas_call(
        spread_kernel,
        out_shape=pltpu.HBM((plane, share, piece), BF16),
        in_specs=[SMEM, HBM],
        out_specs=HBM,
        scratch_shapes=[
            pltpu.VMEM((4, share, piece), BF16),
            pltpu.VMEM((2 * SIDE, share, piece), BF16),
            dma((4,)),
            dma((plane // (2 * SIDE),)),
        ],
        compiler_params=params(4),
        cost_estimate=cost(10**6),
        name="spread",
    )(who, *hbm(output_weight.T))
    eighth = lax.all_to_all(spread, "dp", 0, 0, tiled=True).reshape(model, piece)
    mine = [eighth]
    for o in ((0, 1), (1, 0), (0, -1)):
        mine.append(lax.ppermute(eighth, "dp", from_offset(*o)))
    other = []
    for chunk in mine:
        other.append(lax.ppermute(chunk, "sp", [(i, i ^ 1) for i in range(group)]))

    final, cum = pl.pallas_call(
        summary_kernel,
        out_shape=(
            pltpu.VMEM((group + 1, packed, 128), BF16),
            pltpu.VMEM((tok, width), F32),
        ),
        in_specs=[HBM] * 5,
        out_specs=(VMEM, VMEM),
        scratch_shapes=[
            pltpu.VMEM((tok, width), BF16),
            pltpu.VMEM((tok, width), BF16),
            pltpu.VMEM((tok, heads * vd), BF16),
            pltpu.VMEM(extra_log_decay.shape, F32),
            pltpu.VMEM((heads, kd), F32),
            dma((5,)),
        ],
        compiler_params=params(16),
        cost_estimate=cost(3 * 10**8),
        name="summary",
    )(*hbm(k, x, v, extra_log_decay, decay_offset_bias))

    other_final = lax.ppermute(final, "sp", [(i, i ^ 1) for i in range(group)])
    send = pl.pallas_call(
        combine_kernel,
        out_shape=pltpu.VMEM((group // 2, packed, 128), BF16),
        in_specs=[SMEM, VMEM, VMEM],
        out_specs=VMEM,
        compiler_params=params(8),
        cost_estimate=cost(10**7),
        name="combine",
    )(who, *vmem(final, other_final))
    chips = [[2 * i + c for i in range(group // 2)] for c in range(2)]
    got = lax.all_to_all(send, "sp", 0, 0, axis_index_groups=chips, tiled=True)

    inside, far, own_opening = pl.pallas_call(
        inside_kernel,
        out_shape=(
            pltpu.VMEM((tok, heads * vd), F32),
            pltpu.VMEM((tok, width), BF16),
            pltpu.VMEM((rows, vd), F32),
        ),
        in_specs=[SMEM, VMEM, VMEM] + [HBM] * 4,
        out_specs=(VMEM, VMEM, VMEM),
        scratch_shapes=[
            pltpu.VMEM((tok, width), BF16),
            pltpu.VMEM((tok, width), BF16),
            pltpu.VMEM((tok, heads * vd), BF16),
            dma((4,)),
        ],
        compiler_params=params(16),
        cost_estimate=cost(3 * 10**8),
        name="inside",
    )(who, *vmem(cum, other_final), *hbm(q, k, v, opening))

    starts = pl.pallas_call(
        chain_kernel,
        out_shape=pltpu.VMEM((group, rows, vd), BF16),
        in_specs=[VMEM, VMEM],
        out_specs=VMEM,
        compiler_params=params(8),
        cost_estimate=cost(10**7),
        name="chain",
    )(*vmem(got, own_opening))

    start = lax.all_to_all(starts, "sp", 0, 0, tiled=True)

    out = pl.pallas_call(
        project_kernel,
        out_shape=jax.ShapeDtypeStruct((tok, model), BF16),
        in_specs=[SMEM] + [VMEM] * 3 + [HBM] * 9,
        out_specs=HBM,
        scratch_shapes=[
            pltpu.VMEM((tok, heads * vd), BF16),
            pltpu.VMEM((model, heads * vd), BF16),
            pltpu.VMEM((1, vd), F32),
            pltpu.VMEM((TILES, tok, model // TILES), BF16),
            dma((17,)),
            dma((TILES,)),
        ],
        compiler_params=params(24),
        cost_estimate=cost(10**9),
        name="project",
    )(who, *vmem(inside, far, start), *hbm(output_norm_gain.reshape(1, vd), *mine, *other))
    return out.reshape(tok, seqs, model)


def solution(mesh):
    return jax.shard_map(
        on_device,
        mesh=mesh,
        in_specs=(
            P("sp", "dp", None),
            P("sp", "dp", None),
            P("sp", "dp", None),
            P("sp", "dp", None),
            P("dp", "sp"),
            P(),
            P("dp", None, None, None),
            P(),
            P(None, "dp"),
        ),
        out_specs=P("sp", "dp", None),
        check_vma=False,
    )
```

```python
import jax
import jax.numpy as jnp
from jax import lax
from jax.experimental import pallas as pl
from jax.experimental.pallas import tpu as pltpu
from jax.sharding import PartitionSpec as P


BLOCK = 64
gate_norm_term = 16.0
norm_eps = 1e-05
F32 = jnp.float32
BF16 = jnp.bfloat16
VMEM = pl.BlockSpec(memory_space=pltpu.VMEM)
HBM = pl.BlockSpec(memory_space=pltpu.HBM)
SIDE = 8
TILES = 4


def dot(a, b, dims=(((1,), (0,)), ((), ()))):
    return lax.dot_general(a, b, dims, preferred_element_type=F32)


NT = (((1,), (1,)), ((), ()))
TN = (((0,), (0,)), ((), ()))


def fetch(sems, *pairs):
    copies = [pltpu.make_async_copy(a, b, sems.at[n]) for n, (a, b) in enumerate(pairs)]
    for c in copies:
        c.start()
    return copies


def place():
    sp, dp = lax.axis_index("sp"), lax.axis_index("dp")
    color = lax.rem(lax.rem(dp, SIDE) + 2 * lax.div(dp, SIDE), 4)
    return sp, lax.rem(sp, 2), color


def spread_kernel(weight_hbm, out_hbm, quarters, pattern, sems, out_sems):
    _, core, _ = place()
    width = quarters.shape[2]
    pairs = []
    for c in range(4):
        first = pl.multiple_of((core * 4 + c) * width, width)
        pairs.append((weight_hbm.at[:, pl.ds(first, width)], quarters.at[c]))
    for c in fetch(sems, *pairs):
        c.wait()
    period = pattern.shape[0]
    for d in range(period):
        pattern[d] = quarters[(d % SIDE + 2 * (d // SIDE)) % 4]
    spans = range(0, out_hbm.shape[0], period)
    for c in fetch(out_sems, *[(pattern, out_hbm.at[pl.ds(d, period)]) for d in spans]):
        c.wait()


def summary_kernel(k_hbm, x_hbm, v_hbm, extra_hbm, bias_hbm, send_ref, cum_ref, k_ref, x_ref, v_ref, extra_ref, bias_ref, sems):
    get_x, get_extra, get_bias, get_k, get_v = fetch(
        sems, (x_hbm, x_ref), (extra_hbm, extra_ref), (bias_hbm, bias_ref), (k_hbm, k_ref), (v_hbm, v_ref)
    )
    tok = k_ref.shape[0]
    heads, kd = bias_ref.shape
    vd = v_ref.shape[1] // heads
    per, rows = send_ref.shape[0] // heads, kd * heads // send_ref.shape[0]
    wide = vd // kd
    tri = (
        lax.broadcasted_iota(jnp.int32, (tok, tok), 0)
        >= lax.broadcasted_iota(jnp.int32, (tok, tok), 1)
    ).astype(BF16)
    odd = lax.broadcasted_iota(jnp.int32, (8, kd), 0) % 2 == 1
    get_extra.wait()
    spikes = jnp.transpose(extra_ref[...])
    get_bias.wait()
    get_x.wait()
    for h in range(heads):
        cols = slice(h * kd, (h + 1) * kd)
        x = x_ref[:, cols].astype(F32) + bias_ref[h : h + 1, :]
        log_sig = jnp.minimum(x, 0.0) - jnp.log(1.0 + jnp.exp(-jnp.abs(x)))
        decay = log_sig * (1.0 / gate_norm_term) + spikes[:, h : h + 1]
        high = decay.astype(BF16)
        rest = decay - high.astype(F32)
        mid = rest.astype(BF16)
        low = (rest - mid.astype(F32)).astype(BF16)
        cum = dot(tri, high) + dot(tri, mid) + dot(tri, low)
        cum_ref[:, cols] = cum
        total = cum[tok - 1 : tok, :]
        if h == 0:
            get_k.wait()
            get_v.wait()
        k_out = (k_ref[:, cols].astype(F32) * jnp.exp(total - cum)).astype(BF16)
        final = dot(k_out, v_ref[:, h * vd : (h + 1) * vd], TN).astype(BF16)
        rate = jnp.broadcast_to(jnp.exp(total), (8, kd))
        for r in range(per):
            for w in range(wide):
                send_ref[h * per + r, w * rows : (w + 1) * rows, :] = final[
                    r * rows : (r + 1) * rows, w * kd : (w + 1) * kd
                ]
            turned = pltpu.roll(rate, (kd - r * rows) % kd, 1) if r else rate
            coarse = turned.astype(BF16).astype(F32)
            send_ref[h * per + r, wide * rows : wide * rows + 8, :] = jnp.where(
                odd, turned - coarse, coarse
            ).astype(BF16)


def inside_kernel(
    cum_ref, q_hbm, k_hbm, v_hbm, open_hbm, inside_ref, far_ref, open_ref, q_ref, k_ref, v_ref, sems
):
    mine = open_ref.shape[0]
    first = pl.multiple_of(place()[0] * mine, mine)
    for c in fetch(
        sems, (q_hbm, q_ref), (k_hbm, k_ref), (v_hbm, v_ref), (open_hbm.at[pl.ds(first, mine), :], open_ref)
    ):
        c.wait()
    tok, width = q_ref.shape
    kd = 128
    heads = width // kd
    vd = v_ref.shape[1] // heads
    scale = kd ** (-0.5)
    for h in range(heads):
        cols = slice(h * kd, (h + 1) * kd)
        vcols = slice(h * vd, (h + 1) * vd)
        for i in range(tok // BLOCK):
            lo, hi = i * BLOCK, (i + 1) * BLOCK
            q = q_ref[lo:hi, cols].astype(F32) * scale
            cum = cum_ref[lo:hi, cols]
            far_ref[lo:hi, cols] = (q * jnp.exp(cum)).astype(BF16)
            if i:
                base = cum_ref[lo - 1 : lo, cols]
                q_in = (q * jnp.exp(cum - base)).astype(BF16)
                k_in = (k_ref[0:hi, cols].astype(F32) * jnp.exp(base - cum_ref[0:hi, cols])).astype(BF16)
            else:
                q_in = (q * jnp.exp(cum)).astype(BF16)
                k_in = (k_ref[0:hi, cols].astype(F32) * jnp.exp(-cum)).astype(BF16)
            scores = dot(q_in, k_in, NT)
            seen = (
                lax.broadcasted_iota(jnp.int32, (BLOCK, hi), 0) + lo
                >= lax.broadcasted_iota(jnp.int32, (BLOCK, hi), 1)
            )
            scores = jnp.where(seen, scores, 0.0).astype(BF16)
            inside_ref[lo:hi, vcols] = dot(scores, v_ref[0:hi, vcols])


def chain_kernel(got_ref, open_ref, out_ref):
    group = got_ref.shape[0]
    rows, vd = open_ref.shape
    wide = vd // 128
    where = lax.broadcasted_iota(jnp.int32, (8, 128), 0)
    parts = []
    for g in range(group // 8):
        table = jnp.zeros((8, 128), F32)
        for d in range(8):
            pair = got_ref[g * 8 + d, wide * rows : wide * rows + 8, :].astype(F32)
            table = jnp.where(where == d, pair + pltpu.roll(pair, 1, 0), table)
        parts.append(table)
    rates = jnp.transpose(jnp.concatenate(parts, axis=0))
    states = [open_ref[:, w * 128 : (w + 1) * 128] for w in range(wide)]
    for d in range(group):
        rate = jnp.broadcast_to(rates[0:rows, d : d + 1], (rows, 128))
        for w in range(wide):
            out_ref[d, :, w * 128 : (w + 1) * 128] = states[w].astype(BF16)
            states[w] = rate * states[w] + got_ref[d, w * rows : (w + 1) * rows, :].astype(F32)


def project_kernel(inside_ref, far_ref, start_ref, *refs):
    gain_hbm, mine, other, out_hbm = refs[0], refs[1:5], refs[5:9], refs[9]
    normed, weight, gain_ref, tiles, in_sems, out_sems = refs[10:]
    _, core, color = place()
    half = normed.shape[1] // 2
    piece = half // 4
    model = weight.shape[0]
    heads = 4
    kd, vd = far_ref.shape[1] // heads, start_ref.shape[1]
    halves = 2
    rows = model // halves
    pairs = [(gain_hbm, gain_ref)]
    for part in range(halves):
        span = pl.ds(part * rows, rows)
        for n in range(4):
            at = lax.rem(color + n, 4) * piece
            for base, src in ((core * half, mine[n]), ((1 - core) * half, other[n])):
                to = pl.ds(pl.multiple_of(base + at, piece), piece)
                pairs.append((src.at[span, :], weight.at[span, to]))
    copies = fetch(in_sems, *pairs)
    copies[0].wait()
    for h in range(heads):
        o = inside_ref[:, h * vd : (h + 1) * vd] + dot(
            far_ref[:, h * kd : (h + 1) * kd], start_ref[h * kd : (h + 1) * kd, :]
        )
        spread = lax.rsqrt(jnp.mean(o * o, axis=-1, keepdims=True) + norm_eps)
        normed[:, h * vd : (h + 1) * vd] = (o * spread * gain_ref[...]).astype(BF16)
    tile = model // TILES
    outs = []
    for t in range(TILES):
        if t % (TILES // halves) == 0:
            part = t // (TILES // halves)
            for c in copies[1 + 8 * part : 9 + 8 * part]:
                c.wait()
        tiles[t] = dot(normed[...], weight[t * tile : (t + 1) * tile, :], NT).astype(BF16)
        c = pltpu.make_async_copy(tiles.at[t], out_hbm.at[:, pl.ds(t * tile, tile)], out_sems.at[t])
        c.start()
        outs.append(c)
    for c in outs:
        c.wait()


def hbm(*arrays):
    return [pltpu.with_memory_space_constraint(a, pltpu.HBM) for a in arrays]


def vmem(*arrays):
    return [pltpu.with_memory_space_constraint(a, pltpu.VMEM) for a in arrays]


def params(mib):
    return pltpu.CompilerParams(vmem_limit_bytes=mib * 2**20)


def cost(flops):
    return pl.CostEstimate(flops=flops, bytes_accessed=10**6, transcendentals=0)


def on_device(
    queries,
    head_keys,
    decay_preact,
    values,
    extra_log_decay,
    decay_offset_bias,
    opening_state,
    output_norm_gain,
    output_weight,
):
    tok, seqs, width = queries.shape
    heads, kd = decay_offset_bias.shape
    vd = output_norm_gain.shape[0]
    group = lax.axis_size("sp")
    plane = lax.axis_size("dp")
    share = output_weight.shape[1]
    model = share * plane
    piece = heads * vd // 8
    rows = heads * kd // group
    packed = rows * vd // 128 + 8
    dma = pltpu.SemaphoreType.DMA

    q = queries.reshape(tok, width)
    k = head_keys.reshape(tok, width)
    x = decay_preact.reshape(tok, width)
    v = values.reshape(tok, heads * vd)
    opening = opening_state.reshape(heads * kd, vd)

    def from_offset(dz, dy):
        return [
            (((i + dz) % SIDE) * SIDE + (j + dy) % SIDE, i * SIDE + j)
            for i in range(plane // SIDE)
            for j in range(SIDE)
        ]

    spread = pl.pallas_call(
        spread_kernel,
        out_shape=pltpu.HBM((plane, share, piece), BF16),
        in_specs=[HBM],
        out_specs=HBM,
        scratch_shapes=[
            pltpu.VMEM((4, share, piece), BF16),
            pltpu.VMEM((2 * SIDE, share, piece), BF16),
            dma((4,)),
            dma((plane // (2 * SIDE),)),
        ],
        compiler_params=params(4),
        cost_estimate=cost(10**6),
        name="spread",
    )(*hbm(output_weight.T))
    eighth = lax.all_to_all(spread, "dp", 0, 0, tiled=True).reshape(model, piece)
    mine = [eighth]
    for o in ((0, 1), (1, 0), (0, -1)):
        mine.append(lax.ppermute(eighth, "dp", from_offset(*o)))
    other = []
    for chunk in mine:
        other.append(lax.ppermute(chunk, "sp", [(i, i ^ 1) for i in range(group)]))

    send, cum = pl.pallas_call(
        summary_kernel,
        out_shape=(
            pltpu.VMEM((group, packed, 128), BF16),
            pltpu.VMEM((tok, width), F32),
        ),
        in_specs=[HBM] * 5,
        out_specs=(VMEM, VMEM),
        scratch_shapes=[
            pltpu.VMEM((tok, width), BF16),
            pltpu.VMEM((tok, width), BF16),
            pltpu.VMEM((tok, heads * vd), BF16),
            pltpu.VMEM(extra_log_decay.shape, F32),
            pltpu.VMEM((heads, kd), F32),
            dma((5,)),
        ],
        compiler_params=params(16),
        cost_estimate=cost(3 * 10**8),
        name="summary",
    )(*hbm(k, x, v, extra_log_decay, decay_offset_bias))

    got = lax.all_to_all(send, "sp", 0, 0, tiled=True)

    inside, far, own_opening = pl.pallas_call(
        inside_kernel,
        out_shape=(
            pltpu.VMEM((tok, heads * vd), F32),
            pltpu.VMEM((tok, width), BF16),
            pltpu.VMEM((rows, vd), F32),
        ),
        in_specs=[VMEM] + [HBM] * 4,
        out_specs=(VMEM, VMEM, VMEM),
        scratch_shapes=[
            pltpu.VMEM((tok, width), BF16),
            pltpu.VMEM((tok, width), BF16),
            pltpu.VMEM((tok, heads * vd), BF16),
            dma((4,)),
        ],
        compiler_params=params(16),
        cost_estimate=cost(3 * 10**8),
        name="inside",
    )(*vmem(cum), *hbm(q, k, v, opening))

    starts = pl.pallas_call(
        chain_kernel,
        out_shape=pltpu.VMEM((group, rows, vd), BF16),
        in_specs=[VMEM, VMEM],
        out_specs=VMEM,
        compiler_params=params(8),
        cost_estimate=cost(10**7),
        name="chain",
    )(*vmem(got, own_opening))

    start = lax.all_to_all(starts, "sp", 0, 0, tiled=True).reshape(heads * kd, vd)

    out = pl.pallas_call(
        project_kernel,
        out_shape=jax.ShapeDtypeStruct((tok, model), BF16),
        in_specs=[VMEM] * 3 + [HBM] * 9,
        out_specs=HBM,
        scratch_shapes=[
            pltpu.VMEM((tok, heads * vd), BF16),
            pltpu.VMEM((model, heads * vd), BF16),
            pltpu.VMEM((1, vd), F32),
            pltpu.VMEM((TILES, tok, model // TILES), BF16),
            dma((17,)),
            dma((TILES,)),
        ],
        compiler_params=params(24),
        cost_estimate=cost(10**9),
        name="project",
    )(*vmem(inside, far, start), *hbm(output_norm_gain.reshape(1, vd), *mine, *other))
    return out.reshape(tok, seqs, model)


def solution(mesh):
    return jax.shard_map(
        on_device,
        mesh=mesh,
        in_specs=(
            P("sp", "dp", None),
            P("sp", "dp", None),
            P("sp", "dp", None),
            P("sp", "dp", None),
            P("dp", "sp"),
            P(),
            P("dp", None, None, None),
            P(),
            P(None, "dp"),
        ),
        out_specs=P("sp", "dp", None),
        check_vma=False,
    )
```
